32 devices in a mesh: ep: 8 (over z, core), tp: 4 (over y, x).
Axes of the slice: x: 2, y: 2, z: 4, core: 2. Of those that a mesh axis runs over, the one named last changes fastest.
Arguments:
- tokens: bfloat16 [384, 2048], P('ep', 'tp'), may hold values from -64 to 64
- mix_gain: float32 [2048], replicated, may hold values from 0.1 to 1.9
- w_gate_z: bfloat16 [2048, 2048], P(None, 'tp'), may hold values from -0.125 to 0.125
- w_value_x: bfloat16 [2048, 2048], P(None, 'tp'), may hold values from -0.125 to 0.125
- w_key_b: bfloat16 [2048, 256], replicated, may hold values from -0.125 to 0.125
- w_query_c: bfloat16 [2048, 256], replicated, may hold values from -0.125 to 0.125
- w_step: bfloat16 [2048, 32], replicated, may hold values from -0.125 to 0.125
- step_bias: float32 [32], replicated, may hold values from -2 to 1
- decay_log: float32 [32], replicated, may hold values from -3 to 1.4
- skip_gain: float32 [32], replicated, may hold values from 0.1 to 1.9
- conv_x_weight: bfloat16 [4, 2048], P(None, 'tp'), may hold values from -3 to 3
- conv_b_weight: bfloat16 [4, 256], replicated, may hold values from -3 to 3
- conv_c_weight: bfloat16 [4, 256], replicated, may hold values from -3 to 3
- window_x: bfloat16 [384, 3, 2048], P('ep', None, 'tp'), may hold values from -6 to 6
- window_b: bfloat16 [384, 3, 256], P('ep'), may hold values from -6 to 6
- window_c: bfloat16 [384, 3, 256], P('ep'), may hold values from -6 to 6
- ssm_state: float32 [384, 32, 64, 128], P('ep', 'tp'), may hold values from -2 to 2
- head_gain: float32 [2048], P('tp'), may hold values from 0.1 to 1.9
- w_out: bfloat16 [2048, 2048], P('tp'), may hold values from -0.1875 to 0.1875
- ffn_gain: float32 [2048], replicated, may hold values from 0.1 to 1.9
- route_ids: int32 [384, 2], P('ep'), may hold values from 0 to 31, all different within a row; in each aligned block of 48 rows (0 to 47, 48 to 95, ...) at most 5 rows name the same one
- route_weights: float32 [384, 2], P('ep'), may hold values from 0.05 to 1
- expert_gate: bfloat16 [8, 2048, 4096], P('ep', None, 'tp'), may hold values from -0.125 to 0.125
- expert_up: bfloat16 [8, 2048, 4096], P('ep', None, 'tp'), may hold values from -0.125 to 0.125
- expert_down: bfloat16 [8, 4096, 2048], P('ep', 'tp'), may hold values from -0.25 to 0.25
Outputs:
- layer_out: bfloat16 [384, 2048], P('ep', 'tp')
The draws below stay inside these ranges and needn't reach their ends.
Inputs may be any that keep to these rules, and one draw needn't show every extreme that they name: `route_ids`: each row names 2 different experts. Within the rows of one index of ep (aligned blocks of 48 rows) no expert is named by more than 5 rows, a bound that some block reaches.
All inputs are finite; a program needn't handle non-finite values.
Results may differ from the reference program's by a relative error of at most 0.009.
Values may be sent and summed in bfloat16 or wider, within the bound.
A program may use at most 64 MiB of HBM per device.

```python
import math
import jax
import jax.numpy as jnp
import numpy as np
from jax import lax

D = 2048
HEADS = 32
HEAD_DIM = 64
STATE = 128
GROUPS = 2
CONV = 4
FE = 1024
EXP_IN = 4
TOPK = 2
SEQ_DEV = 48
SSD_W = 2048
GN = 256
SEQS = 384
SETS = 8
EXPERTS = 32
SET_UNITS = 4096
CAP = 5
N_EP = 8


def draw_tokens(key, part):
    base_key = jax.random.fold_in(key, 11)
    row_key, column_key, body_key = jax.random.split(base_key, 3)
    row_scale = jnp.exp(jax.random.uniform(row_key, (SEQS, 1), jnp.float32, math.log(0.3), math.log(3.0)))
    column_scale = jnp.exp(jax.random.uniform(column_key, (1, D), jnp.float32, math.log(0.3), math.log(3.0)))
    pattern = jax.random.normal(body_key, (SEQS, D), jnp.float32)
    pattern = jnp.clip(pattern, -6.0, 6.0)
    return (pattern * row_scale * column_scale).astype(jnp.bfloat16)


def raised(entries, stream_key, source, target, shards_of, factor):
    owner, partner = [(jnp.arange(entries.shape[axis_at]) // (entries.shape[axis_at] // shards_of)).reshape([-1 if axis == axis_at else 1 for axis in range(entries.ndim)]) for axis_at in (source, target)]
    chosen = jax.random.permutation(stream_key, shards_of)[partner]
    strong = (owner == chosen) | (owner == (partner + shards_of // 2) % shards_of)
    return jnp.where(strong, factor * entries, entries)


def steps_of(rng, dims, shards, low, top_value):
    factor_of = 1.0
    for axis_at, parts in shards:
        heights = jax.random.uniform(jax.random.fold_in(jax.random.fold_in(rng, 6), axis_at), (parts,), jnp.float32, low / len(shards), top_value / len(shards))
        factor_of = factor_of * jnp.repeat(jnp.exp(heights), dims[axis_at] // parts).reshape((-1,) + (1,) * (len(dims) - 1 - axis_at))
    return factor_of


def deal_out(stream_key, own, number, rows, number_of, top, bound, slope):
    ranking = jax.random.permutation(stream_key, number_of)
    crowded, usual = load_shares(number_of, rows * top, bound, slope, True), load_shares(number_of, rows * top, bound, slope, False)
    places = jnp.arange(number_of)

    def named(lengths, offset_by):
        used = int((lengths > 0).sum())
        fixed = max(1, used // 4)
        moved = fixed + (places - fixed + offset_by * (used - fixed)) % max(1, number_of - fixed)
        return jnp.zeros((number_of,), jnp.int32).at[ranking[jnp.where(places < fixed, places, moved)]].set(jnp.asarray(lengths, jnp.int32))

    lengths = jnp.where(number % 4 == 0, named(crowded, number // 4), named(usual, number - number // 4 - 1))
    mixed = jax.random.permutation(jax.random.fold_in(own, 3), number_of)
    source_of, taker = mixed[0:number_of // 2 * 2:2], mixed[1:number_of // 2 * 2:2]
    margin = jnp.minimum(lengths[source_of] - 1, bound - lengths[taker]) // 2
    margin = jnp.where((source_of == ranking[0]) | (taker == ranking[0]) | (lengths[taker] == 0), 0, jnp.maximum(margin, 0))
    moved = jax.random.randint(jax.random.fold_in(own, 4), (number_of // 2,), 0, 1 << 20) % (margin + 1)
    lengths = lengths.at[source_of].add(-moved).at[taker].add(moved)
    labels = jnp.searchsorted(jnp.cumsum(lengths), jnp.arange(rows * top), side="right").astype(jnp.int32)
    table = labels.reshape(top, rows).T
    table = table[jax.random.permutation(jax.random.fold_in(own, 1), rows)]
    offset_by = jax.random.randint(jax.random.fold_in(own, 2), (rows, 1), 0, top)
    return jnp.take_along_axis(table, (jnp.arange(top)[None, :] + offset_by) % top, axis=1)


def load_shares(amount, total, reach, lean, full):
    portions = [(1 << 20) // math.isqrt(rank ** lean) + 1 for rank in range(1, amount + 1)]
    largest = reach if full else min(reach, max(-(-total // amount), total * portions[0] // sum(portions)))
    least = 1 if total - largest >= amount - 1 else 0
    given, rest = [largest] + [least] * (amount - 1), total - largest - least * (amount - 1)
    while rest > 0:
        free = [i for i in range(1, amount) if given[i] < largest] or [i for i in range(1, amount) if given[i] < reach]
        mass, left = sum([portions[i] for i in free]), rest
        for i in free:
            addition = min(reach - given[i], max(1, left * portions[i] // mass), rest)
            given[i] = given[i] + addition
            rest = rest - addition
    return np.array(given)


def noise(own_key, dims, width, limit, shards=(), kind=jnp.bfloat16):
    array = jax.random.normal(own_key, dims, jnp.float32) * width
    if len(shards) > 0:
        array = steps_of(own_key, dims, shards, -0.22, 0.18) * array
    return jnp.clip(array, min=-limit, max=limit).astype(kind)


def heavy_noise(stream_key, extent, spread, reach, pieces, heavy, held_as=jnp.bfloat16):
    entries = spread * jax.random.normal(stream_key, extent, jnp.float32)
    if pieces:
        entries = entries * steps_of(stream_key, extent, pieces, -0.22, 0.18)
    return jnp.clip(raised(entries, jax.random.fold_in(stream_key, 3), *heavy), -reach, reach).astype(held_as)


def setup_inputs(seed: int = 0) -> dict:
    arg_keys = jax.random.split(jax.random.key(seed), 26)
    tokens = draw_tokens(jax.random.fold_in(arg_keys[25], 71), 0)
    mix_gain = jnp.clip(1.0 + 0.18 * jax.random.normal(arg_keys[1], (D,), jnp.float32), 0.1, 1.9)
    w_gate_z = noise(arg_keys[2], (D, SSD_W), D ** -0.5, 0.125, ((1, 4),))
    w_value_x = noise(arg_keys[3], (D, SSD_W), D ** -0.5, 0.125, ((1, 4),))
    w_key_b = noise(arg_keys[4], (D, GN), D ** -0.5, 0.125)
    w_query_c = noise(arg_keys[5], (D, GN), D ** -0.5, 0.125)
    w_step = noise(arg_keys[6], (D, HEADS), D ** -0.5, 0.125)
    step_bias = jnp.clip(jax.random.uniform(arg_keys[7], (HEADS,), jnp.float32, -2.0, 1.0), -2.0, 1.0)
    decay_log = jnp.clip(jax.random.uniform(arg_keys[8], (HEADS,), jnp.float32, -3.0, 1.4), -3.0, 1.4)
    skip_gain = jnp.clip(1.0 + 0.18 * jax.random.normal(arg_keys[9], (HEADS,), jnp.float32), 0.1, 1.9)
    conv_x_weight = noise(arg_keys[10], (CONV, SSD_W), CONV ** -0.5, 3.0, ((1, 4),))
    conv_b_weight = noise(arg_keys[11], (CONV, GN), CONV ** -0.5, 3.0)
    conv_c_weight = noise(arg_keys[12], (CONV, GN), CONV ** -0.5, 3.0)
    window_x = noise(arg_keys[13], (SEQS, CONV - 1, SSD_W), 1.0, 6.0, ((0, 8), (2, 4)))
    window_b = noise(arg_keys[14], (SEQS, CONV - 1, GN), 1.0, 6.0, ((0, 8),))
    window_c = noise(arg_keys[15], (SEQS, CONV - 1, GN), 1.0, 6.0, ((0, 8),))
    ssm_state = noise(arg_keys[16], (SEQS, HEADS, HEAD_DIM, STATE), 0.3, 2.0, ((0, 8), (1, 4)), jnp.float32)
    head_gain = jnp.clip(1.0 + 0.18 * jax.random.normal(arg_keys[17], (SSD_W,), jnp.float32), 0.1, 1.9)
    w_out = heavy_noise(arg_keys[18], (SSD_W, D), SSD_W ** -0.5, 0.1875, ((0, 4),), (0, 1, 4, 2.0))
    ffn_gain = jnp.clip(1.0 + 0.18 * jax.random.normal(arg_keys[19], (D,), jnp.float32), 0.1, 1.9)
    route_ids_keys = jax.random.split(jax.random.fold_in(arg_keys[20], 1), SEQS // SEQ_DEV)
    route_ids_turns = jax.random.permutation(jax.random.fold_in(arg_keys[20], 3), SEQS // SEQ_DEV)
    route_ids = jax.vmap(lambda own, number: deal_out(jax.random.fold_in(arg_keys[20], 2), own, number, SEQ_DEV, EXPERTS, TOPK, CAP, 2))(route_ids_keys, route_ids_turns).reshape((SEQS, TOPK))
    route_weights = jnp.clip(0.05 + 0.95 * jax.random.uniform(arg_keys[21], (SEQS, TOPK), jnp.float32) ** steps_of(arg_keys[21], (SEQS, TOPK), ((0, 8),), -0.2, 0.2), 0.05, 1.0)
    expert_gate = noise(arg_keys[22], (SETS, D, SET_UNITS), D ** -0.5, 0.125, ((0, 8), (2, 4)))
    expert_up = noise(arg_keys[23], (SETS, D, SET_UNITS), D ** -0.5, 0.125, ((0, 8), (2, 4)))
    expert_down = heavy_noise(arg_keys[24], (SETS, SET_UNITS, D), FE ** -0.5, 0.25, ((0, 8), (1, 4)), (1, 2, 4, 2.0))
    return {"tokens": tokens, "mix_gain": mix_gain, "w_gate_z": w_gate_z, "w_value_x": w_value_x, "w_key_b": w_key_b, "w_query_c": w_query_c, "w_step": w_step, "step_bias": step_bias, "decay_log": decay_log, "skip_gain": skip_gain, "conv_x_weight": conv_x_weight, "conv_b_weight": conv_b_weight, "conv_c_weight": conv_c_weight, "window_x": window_x, "window_b": window_b, "window_c": window_c, "ssm_state": ssm_state, "head_gain": head_gain, "w_out": w_out, "ffn_gain": ffn_gain, "route_ids": route_ids, "route_weights": route_weights, "expert_gate": expert_gate, "expert_up": expert_up, "expert_down": expert_down}


norm_epsilon = 1e-06

def row_norm(arr_values, norm_gain):
    widened = arr_values.astype(jnp.float32)
    return widened * lax.rsqrt(lax.optimization_barrier(jnp.mean(widened * widened, axis=-1, keepdims=True)) + norm_epsilon) * norm_gain

def short_conv(window, fresh_row, weight):
    conv_taps = weight.astype(jnp.float32)
    summed = lax.optimization_barrier(jnp.sum(window.astype(jnp.float32) * conv_taps[:-1][None], axis=1)) + fresh_row * conv_taps[-1]
    return jax.nn.silu(summed)

def product(left, right):
    return jnp.dot(left, right, preferred_element_type=jnp.float32)

def reference(tokens, mix_gain, w_gate_z, w_value_x, w_key_b, w_query_c, w_step, step_bias, decay_log, skip_gain, conv_x_weight, conv_b_weight, conv_c_weight, window_x, window_b, window_c, ssm_state, head_gain, w_out, ffn_gain, route_ids, route_weights, expert_gate, expert_up, expert_down):
    seq_count = tokens.shape[0]
    normed = row_norm(tokens, mix_gain).astype(jnp.bfloat16)
    gate_z = product(normed, w_gate_z)
    values = short_conv(window_x, product(normed, w_value_x), conv_x_weight)
    keys = short_conv(window_b, product(normed, w_key_b), conv_b_weight)
    queries = short_conv(window_c, product(normed, w_query_c), conv_c_weight)
    step_size = jax.nn.softplus(product(normed, w_step) + step_bias)
    decay_heads = jnp.exp(-step_size * jnp.exp(decay_log))
    per_group = HEADS // GROUPS
    value_heads = values.reshape(seq_count, HEADS, HEAD_DIM)
    key_heads = jnp.repeat(keys.reshape(seq_count, GROUPS, STATE), per_group, axis=1)
    query_heads = jnp.repeat(queries.reshape(seq_count, GROUPS, STATE), per_group, axis=1)
    new_state = decay_heads[:, :, None, None] * ssm_state + (step_size[:, :, None] * value_heads)[..., None] * key_heads[:, :, None, :]
    read_out = jnp.einsum('shpn,shn->shp', new_state, query_heads, precision=lax.Precision.HIGHEST)
    read_out = read_out + skip_gain[None, :, None] * value_heads
    gated = read_out * jax.nn.silu(gate_z.reshape(seq_count, HEADS, HEAD_DIM))
    gated = gated * lax.rsqrt(lax.optimization_barrier(jnp.mean(gated * gated, axis=-1, keepdims=True)) + norm_epsilon)
    mixed_heads = (gated * head_gain.reshape(HEADS, HEAD_DIM)).reshape(seq_count, SSD_W).astype(jnp.bfloat16)
    mix_out = product(mixed_heads, w_out)
    residual = (tokens.astype(jnp.float32) + mix_out).astype(jnp.bfloat16)
    ffn_in = row_norm(residual, ffn_gain).astype(jnp.bfloat16)
    route_share = route_weights / lax.optimization_barrier(jnp.sum(route_weights, axis=1, keepdims=True))
    rows_most = N_EP * CAP
    row_order = jnp.arange(seq_count, dtype=jnp.int32)
    zero_index = jnp.zeros((), jnp.int32)

    def one_expert(running, expert):
        hit_mask = route_ids == expert
        weight = lax.optimization_barrier(jnp.sum(jnp.where(hit_mask, route_share, 0.0), axis=1))
        taken_rows = jnp.any(hit_mask, axis=1)
        rank_key = jnp.where(taken_rows, 0, seq_count).astype(jnp.int32) + row_order
        picked = jnp.argsort(rank_key)[:rows_most].astype(jnp.int32)
        chosen_rows = ffn_in[picked]
        set_index = (expert // EXP_IN).astype(jnp.int32)
        sub_start = (expert % EXP_IN * FE).astype(jnp.int32)
        gate_block = lax.dynamic_slice(expert_gate, (set_index, zero_index, sub_start), (1, D, FE))[0]
        up_block = lax.dynamic_slice(expert_up, (set_index, zero_index, sub_start), (1, D, FE))[0]
        down_block = lax.dynamic_slice(expert_down, (set_index, sub_start, zero_index), (1, FE, D))[0]
        hidden = (jax.nn.silu(product(chosen_rows, gate_block)) * product(chosen_rows, up_block)).astype(jnp.bfloat16)
        result = product(hidden, down_block)
        running = running.at[picked].add(weight[picked][:, None] * result)
        return (running, None)
    moe_sum, unused = lax.scan(one_expert, jnp.zeros((seq_count, D), jnp.float32), jnp.arange(EXPERTS, dtype=jnp.int32))
    return (residual.astype(jnp.float32) + moe_sum).astype(jnp.bfloat16)
```

```python
import functools

import jax
import jax.numpy as jnp
from jax import lax
from jax.experimental import pallas as pl
from jax.experimental.pallas import tpu as pltpu
from jax.sharding import PartitionSpec as P

HEADS = 32
HEAD_DIM = 64
STATE = 128
GROUPS = 2
EXP_IN = 4


norm_epsilon = 1e-06


def row_norm(arr_values, norm_gain):
    widened = arr_values.astype(jnp.float32)
    return (
        widened
        * lax.rsqrt(jnp.mean(widened * widened, axis=-1, keepdims=True) + norm_epsilon)
        * norm_gain
    )


def short_conv(window, fresh_row, weight):
    conv_taps = weight.astype(jnp.float32)
    summed = (
        jnp.sum(window.astype(jnp.float32) * conv_taps[:-1][None], axis=1)
        + fresh_row * conv_taps[-1]
    )
    return jax.nn.silu(summed)


def product(left, right):
    return jnp.dot(left, right, preferred_element_type=jnp.float32)


def local_plain(
    tokens,
    mix_gain,
    w_gate_z,
    w_value_x,
    w_key_b,
    w_query_c,
    w_step,
    step_bias,
    decay_log,
    skip_gain,
    conv_x_weight,
    conv_b_weight,
    conv_c_weight,
    window_x,
    window_b,
    window_c,
    ssm_state,
    head_gain,
    w_out,
    ffn_gain,
    route_ids,
    route_weights,
    expert_gate,
    expert_up,
    expert_down,
):
    tp_index = lax.axis_index("tp")
    tp_count = lax.axis_size("tp")
    ep_count = lax.axis_size("ep")
    seq_count = tokens.shape[0]
    gathered = lax.all_gather(tokens, "tp", axis=1, tiled=True)
    normed = row_norm(gathered, mix_gain).astype(jnp.bfloat16)
    local_width = w_gate_z.shape[1]
    head_count = local_width // HEAD_DIM
    first_head = tp_index * head_count
    group_start = first_head // (HEADS // GROUPS) * STATE
    gate_z = product(normed, w_gate_z)
    values = short_conv(window_x, product(normed, w_value_x), conv_x_weight)
    key_b = short_conv(
        lax.dynamic_slice_in_dim(window_b, group_start, STATE, 2),
        product(normed, lax.dynamic_slice_in_dim(w_key_b, group_start, STATE, 1)),
        lax.dynamic_slice_in_dim(conv_b_weight, group_start, STATE, 1),
    )
    query_c = short_conv(
        lax.dynamic_slice_in_dim(window_c, group_start, STATE, 2),
        product(normed, lax.dynamic_slice_in_dim(w_query_c, group_start, STATE, 1)),
        lax.dynamic_slice_in_dim(conv_c_weight, group_start, STATE, 1),
    )
    step_all = product(normed, w_step) + step_bias
    step_size = jax.nn.softplus(lax.dynamic_slice_in_dim(step_all, first_head, head_count, 1))
    rate_heads = jnp.exp(lax.dynamic_slice_in_dim(decay_log, first_head, head_count, 0))
    skip_heads = lax.dynamic_slice_in_dim(skip_gain, first_head, head_count, 0)
    decay_heads = jnp.exp(-step_size * rate_heads)
    value_heads = values.reshape(seq_count, head_count, HEAD_DIM)
    new_state = (
        decay_heads[:, :, None, None] * ssm_state
        + (step_size[:, :, None] * value_heads)[..., None] * key_b[:, None, None, :]
    )
    read_out = jnp.einsum("shpn,sn->shp", new_state, query_c, precision=lax.Precision.HIGHEST)
    read_out = read_out + skip_heads[None, :, None] * value_heads
    gated = read_out * jax.nn.silu(gate_z.reshape(seq_count, head_count, HEAD_DIM))
    gated = gated * lax.rsqrt(jnp.mean(gated * gated, axis=-1, keepdims=True) + norm_epsilon)
    mixed_heads = (
        (gated * head_gain.reshape(head_count, HEAD_DIM))
        .reshape(seq_count, local_width)
        .astype(jnp.bfloat16)
    )
    partial_value = product(mixed_heads, w_out)
    share_mix = lax.psum_scatter(partial_value, "tp", scatter_dimension=1, tiled=True)
    residual_own = (tokens.astype(jnp.float32) + share_mix).astype(jnp.bfloat16)
    residual_full = lax.all_gather(residual_own, "tp", axis=1, tiled=True)
    ffn_in = row_norm(residual_full, ffn_gain).astype(jnp.bfloat16)
    top_count = route_ids.shape[1]
    expert_count = EXP_IN * ep_count
    capacity = max(2, (3 * seq_count * top_count + 2 * expert_count - 1) // (2 * expert_count))
    sub_index = tp_index // (tp_count // EXP_IN)
    target_set = route_ids // EXP_IN
    hit_mask = route_ids % EXP_IN == sub_index
    set_grid = jnp.arange(ep_count, dtype=jnp.int32)
    set_onehot = (hit_mask[:, :, None] & (target_set[:, :, None] == set_grid)).astype(jnp.int32)
    set_onehot = set_onehot.reshape(seq_count * top_count, ep_count)
    earlier = jnp.cumsum(set_onehot, axis=0) - set_onehot
    slot_rank = jnp.sum(earlier * set_onehot, axis=1).reshape(seq_count, top_count)
    slot_index = jnp.where(hit_mask, target_set * capacity + slot_rank, -1)
    slot_grid = jnp.arange(ep_count * capacity, dtype=jnp.int32)
    slot_match = slot_index[:, :, None] == slot_grid
    placed = jnp.any(slot_match, axis=1).astype(jnp.bfloat16)
    outgoing = jnp.einsum("sj,sd->jd", placed, ffn_in, preferred_element_type=jnp.float32)
    outgoing = outgoing.astype(jnp.bfloat16).reshape(ep_count, capacity, ffn_in.shape[1])
    route_share = route_weights / jnp.sum(route_weights, axis=1, keepdims=True)
    combine_weight = jnp.sum(jnp.where(slot_match, route_share[:, :, None], 0.0), axis=1)
    arrived = lax.all_to_all(outgoing, "ep", split_axis=0, concat_axis=0, tiled=True)
    source_count, slot_count, row_width = arrived.shape
    flat_rows = arrived.reshape(source_count * slot_count, row_width)
    gate_part = product(flat_rows, expert_gate[0])
    up_part = product(flat_rows, expert_up[0])
    hidden = (jax.nn.silu(gate_part) * up_part).astype(jnp.bfloat16)
    expert_out = product(hidden, expert_down[0]).reshape(source_count, slot_count, row_width)
    returned = lax.all_to_all(
        expert_out.astype(jnp.bfloat16), "ep", split_axis=0, concat_axis=0, tiled=True
    ).astype(expert_out.dtype)
    moe_part = jnp.dot(
        combine_weight,
        returned.reshape(ep_count * capacity, -1),
        precision=lax.Precision.HIGHEST,
        preferred_element_type=jnp.float32,
    )
    moe_share = lax.psum_scatter(
        moe_part.astype(jnp.bfloat16), "tp", scatter_dimension=1, tiled=True
    ).astype(jnp.float32)
    return (residual_own.astype(jnp.float32) + moe_share).astype(jnp.bfloat16)


MESH = pl.DeviceIdType.MESH
HIGH = lax.Precision.HIGHEST
BF = jnp.bfloat16
F32 = jnp.float32
LANES = 128
TILE = 256


def silu(v):
    return v / (1.0 + jnp.exp(-v))


def dot32(left, right, precision=None):
    return jnp.dot(left, right, preferred_element_type=F32, precision=precision)


def dot32_t(left, right):
    return lax.dot_general(left, right, (((1,), (1,)), ((), ())), preferred_element_type=F32)


def halves(v):
    high = v.astype(BF)
    return high, (v - high.astype(F32)).astype(BF)


def split_index(index, *counts):
    digits = []
    for place in range(len(counts) - 1):
        below = 1
        for count in counts[place + 1 :]:
            below = below * count
        digit = jnp.zeros_like(index)
        for step in range(1, counts[place]):
            digit = digit + jnp.where(index >= step * below, 1, 0)
        index = index - digit * below
        digits.append(digit)
    return (*digits, index)


_open = []


def mark(name):
    if _open:
        _open.pop().__exit__(None, None, None)
    if name:
        scope = jax.named_scope(name)
        scope.__enter__()
        _open.append(scope)


def layer_entry(n_ep, n_tp, slots, n_small, *refs):
    held, small_sem = refs[-1 - n_small : -1], refs[-1]
    fetches = [
        pltpu.make_async_copy(refs[at], held[at], small_sem.at[at]) for at in range(n_small)
    ]
    layer_kernel(n_ep, n_tp, slots, fetches, *held, *refs[n_small : -1 - n_small])


def layer_kernel(
    n_ep,
    n_tp,
    slots,
    fetches,
    tokens,
    mix_gain,
    step_bias,
    decay_log,
    skip_gain,
    conv_x,
    conv_b,
    conv_c,
    window_x,
    window_b,
    window_c,
    head_gain,
    ffn_gain,
    ids_t,
    scores_t,
    hbm_gate_z,
    hbm_value_x,
    hbm_key_b,
    hbm_query_c,
    hbm_step,
    hbm_state,
    hbm_out,
    hbm_exp_gate,
    hbm_exp_up,
    hbm_exp_down,
    out,
    w_gate_z,
    w_value_x,
    w_key_b,
    w_query_c,
    w_step,
    state,
    w_out,
    exp_gate,
    exp_up,
    exp_down,
    gathered,
    normed,
    queries,
    state_read,
    mix_send,
    mix_recv,
    row_send,
    row_recv,
    place,
    comb_high,
    comb_low,
    pick,
    unpick,
    sum_egate,
    sum_eup,
    hidden,
    back_send,
    back_recv,
    load_sem,
    state_sem,
    tok_send_sem,
    tok_recv_sem,
    mix_send_sem,
    mix_recv_sem,
    row_send_sem,
    row_recv_sem,
    back_send_sem,
    back_recv_sem,
):
    me_e = lax.axis_index("ep")
    me_t = lax.axis_index("tp")
    seqs, width = tokens.shape
    features = width * n_tp
    tiles = width // LANES
    lines = tiles * slots
    n_lines = n_ep * lines
    n_rows = n_ep * slots
    heads_here = width // HEAD_DIM
    first_head = me_t * heads_here
    group_start = pl.multiple_of(first_head // (HEADS // GROUPS) * STATE, STATE)
    group_cols = pl.ds(group_start, STATE)
    state_blocks = state_sem.shape[0]
    state_rows = seqs // state_blocks

    def peer(step):
        row, column = me_t // 2, lax.rem(me_t, 2)
        return lax.rem(row + step // 2, 2) * 2 + lax.rem(column + step % 2, 2)

    def other_e(step):
        return lax.rem(me_e + step, n_ep)

    far_first = sorted(range(n_ep), key=lambda step: -min(step, n_ep - step))
    steps = tuple(reversed(range(n_tp)))

    def load(source, target, index):
        return pltpu.make_async_copy(source, target, load_sem.at[index])

    load_key = load(hbm_key_b.at[:, group_cols], w_key_b, 0)
    load_query = load(hbm_query_c.at[:, group_cols], w_query_c, 1)
    load_step = load(hbm_step, w_step, 2)
    load_value = load(hbm_value_x, w_value_x, 3)
    load_gate = load(hbm_gate_z, w_gate_z, 4)
    load_out = load(hbm_out, w_out, 5)
    load_exp_gate = load(hbm_exp_gate, exp_gate, 6)
    load_exp_up = load(hbm_exp_up, exp_up, 7)
    load_exp_down = load(hbm_exp_down, exp_down, 8)

    def load_state(block):
        rows = pl.ds(block * state_rows, state_rows)
        return pltpu.make_async_copy(hbm_state.at[rows], state.at[rows], state_sem.at[block])

    mark("greet")
    for each in fetches:
        each.start()
    barrier = pltpu.get_barrier_semaphore()
    for step in range(1, n_tp):
        pl.semaphore_signal(
            barrier, inc=1, device_id=(me_e, peer(step)), device_id_type=MESH
        )
    for step in far_first:
        if step:
            pl.semaphore_signal(
                barrier, inc=1, device_id=(other_e(step), me_t), device_id_type=MESH
            )
    mark("loads")
    for each in (load_query, load_key, load_step, load_value, load_gate):
        each.start()
    for block in range(state_blocks):
        load_state(block).start(priority=1)
    mark("smallwait")
    for each in fetches:
        each.wait()
    mark("barrier")
    pl.semaphore_wait(barrier, n_tp + n_ep - 2)
    mark("toksend")

    def token_copy(step):
        return pltpu.make_async_remote_copy(
            src_ref=tokens,
            dst_ref=gathered.at[step - 1],
            send_sem=tok_send_sem,
            recv_sem=tok_recv_sem.at[step - 1],
            device_id=(me_e, peer(step)),
            device_id_type=MESH,
        )

    for step in reversed(range(1, n_tp)):
        token_copy(step).start()

    def part_rows(step):
        return pl.ds(pl.multiple_of(peer(step) * width, width), width)

    def squares_of(piece):
        wide = piece.astype(F32)
        return jnp.sum(wide * wide, axis=1, keepdims=True)

    mark("routes")
    n_exp = n_ep * EXP_IN
    row_at = lax.broadcasted_iota(jnp.int32, (seqs, seqs), 0)
    col_at = lax.broadcasted_iota(jnp.int32, (seqs, seqs), 1)

    def stood_up(row):
        return jnp.sum(jnp.where(row_at == col_at, row, 0.0), axis=1, keepdims=True)

    id0 = stood_up(ids_t[0:1, :].astype(F32)).astype(jnp.int32)
    id1 = stood_up(ids_t[1:2, :].astype(F32)).astype(jnp.int32)
    lane_exp = lax.broadcasted_iota(jnp.int32, (seqs, n_exp), 1)
    hit0 = jnp.where(id0 == lane_exp, 1.0, 0.0)
    hit1 = jnp.where(id1 == lane_exp, 1.0, 0.0)
    lower = jnp.where(row_at > col_at, 1.0, 0.0).astype(BF)
    upper = jnp.where(row_at < col_at, 1.0, 0.0).astype(BF)
    before = dot32(lower, (hit0 + hit1).astype(BF))
    slot0 = id0 * slots + jnp.sum(before * hit0, axis=1, keepdims=True).astype(jnp.int32)
    slot1 = id1 * slots + jnp.sum(before * hit1, axis=1, keepdims=True).astype(jnp.int32)
    score0, score1 = stood_up(scores_t[0:1, :]), stood_up(scores_t[1:2, :])
    total = score0 + score1

    def stacked(column):
        return jnp.concatenate([column] * tiles, axis=0)

    slot0, slot1 = stacked(slot0), stacked(slot1)
    share0, share1 = stacked(score0 / total), stacked(score1 / total)

    idt0, idt1 = ids_t[0:1, :], ids_t[1:2, :]
    sub_exp = lax.broadcasted_iota(jnp.int32, (n_exp, seqs), 0)
    hitt0 = jnp.where(idt0 == sub_exp, 1.0, 0.0)
    hitt1 = jnp.where(idt1 == sub_exp, 1.0, 0.0)
    before_t = dot32((hitt0 + hitt1).astype(BF), upper)
    rank0 = jnp.sum(before_t * hitt0, axis=0, keepdims=True)
    rank1 = jnp.sum(before_t * hitt1, axis=0, keepdims=True)
    rep_row = lax.broadcasted_iota(jnp.int32, (seqs, tiles * seqs), 0)
    rep_col = lax.broadcasted_iota(jnp.int32, (1, tiles * seqs), 1)
    tile_col, token_col = split_index(rep_col, tiles, seqs)
    repeat = jnp.where(rep_row == token_col, 1.0, 0.0).astype(BF)
    wide_ids = dot32(
        jnp.concatenate([idt0.astype(F32), idt1.astype(F32), rank0, rank1] * 2, axis=0).astype(BF),
        repeat,
    ).astype(jnp.int32)
    slott0 = wide_ids[0:1, :] * slots + wide_ids[2:3, :]
    slott1 = wide_ids[1:2, :] * slots + wide_ids[3:4, :]

    line_row = lax.broadcasted_iota(jnp.int32, (n_lines, 1), 0)
    e_row, c_row, k_row = split_index(line_row, n_ep, tiles, slots)
    line_col = lax.broadcasted_iota(jnp.int32, (1, n_lines), 1)
    e_col, c_col, k_col = split_index(line_col, n_ep, tiles, slots)
    tok_row = lax.broadcasted_iota(jnp.int32, (tiles * seqs, 1), 0)
    tile_row, _ = split_index(tok_row, tiles, seqs)
    pick[...] = jnp.where(
        line_row == c_col * n_rows + e_col * slots + k_col, 1.0, 0.0
    ).astype(BF)
    unpick[...] = jnp.where(
        line_col == c_row * n_rows + e_row * slots + k_row, 1.0, 0.0
    ).astype(BF)
    for step in range(n_tp):
        there_row = (e_row * n_tp + peer(step)) * slots + k_row
        there_col = (e_col * n_tp + peer(step)) * slots + k_col
        same = c_row == tile_col
        chosen = same & ((slott0 == there_row) | (slott1 == there_row))
        place[step] = jnp.where(chosen, 1.0, 0.0).astype(BF)
        same = tile_row == c_col
        weight = jnp.where(same & (slot0 == there_col), share0, 0.0) + jnp.where(
            same & (slot1 == there_col), share1, 0.0
        )
        comb_high[step], comb_low[step] = halves(weight)

    mark("pasts")

    def window_sum(window, taps, columns):
        summed = None
        for tap in range(window.shape[0]):
            term = window[tap, :, columns].astype(F32) * taps[tap : tap + 1, :]
            summed = term if summed is None else summed + term
        return summed

    every = pl.ds(0, width)
    taps_x = conv_x[...].astype(F32)
    taps_b = conv_b[:, group_cols].astype(F32)
    taps_c = conv_c[:, group_cols].astype(F32)
    last = taps_x.shape[0] - 1
    past_x = window_sum(window_x, taps_x, every)
    past_b = window_sum(window_b, taps_b, group_cols)
    past_c = window_sum(window_c, taps_c, group_cols)
    head_row = lax.broadcasted_iota(jnp.int32, (HEADS, width), 0)
    head_col = lax.broadcasted_iota(jnp.int32, (HEADS, width), 1) // HEAD_DIM + first_head
    spread = jnp.where(head_row == head_col, 1.0, 0.0).astype(BF)
    same_row = lax.rem(lax.broadcasted_iota(jnp.int32, (2 * LANES, LANES), 0), LANES) // HEAD_DIM
    same_col = lax.broadcasted_iota(jnp.int32, (2 * LANES, LANES), 1) // HEAD_DIM
    same_head = jnp.where(same_row == same_col, 1.0, 0.0).astype(BF)
    skip = dot32(jnp.broadcast_to(skip_gain[...], (8, HEADS)), spread.astype(F32), HIGH)[0:1, :]

    squares = squares_of(tokens[...])
    for step in range(1, n_tp):
        mark(f"tokwait{step}")
        token_copy(step).wait_recv()
        squares = squares + squares_of(gathered[step - 1])
    mark("norm")
    for each in (load_out, load_exp_gate, load_exp_up, load_exp_down):
        each.start(priority=1)
    scale = lax.rsqrt(squares / features + norm_epsilon)
    for step in range(n_tp):
        piece = gathered[step - 1] if step else tokens[...]
        columns = part_rows(step)
        normed[:, columns] = (piece.astype(F32) * scale * mix_gain[:, columns]).astype(BF)
    mark("projwait")
    for each in (load_query, load_key, load_step, load_value, load_gate):
        each.wait()
    mark("query")
    query = silu(past_c + dot32(normed[...], w_query_c[...]) * taps_c[last : last + 1, :])
    queries[...] = query
    key = silu(past_b + dot32(normed[...], w_key_b[...]) * taps_b[last : last + 1, :])
    key_query = jnp.sum(key * query, axis=1, keepdims=True)
    raw_step = dot32_t(normed[...], w_step[...]) + step_bias[...]
    step_size = jnp.maximum(raw_step, 0.0) + jnp.log1p(jnp.exp(-jnp.abs(raw_step)))
    decay = jnp.exp(-step_size * jnp.exp(decay_log[...]))
    spread_high, spread_low = halves(jnp.concatenate([step_size, decay], axis=0))
    wide = dot32(jnp.concatenate([spread_high, spread_low], axis=0), spread)
    step_wide = wide[0:seqs] + wide[2 * seqs : 3 * seqs]
    decay_wide = wide[seqs : 2 * seqs] + wide[3 * seqs : 4 * seqs]
    mark("value")
    values = silu(past_x + dot32(normed[...], w_value_x[...]) * taps_x[last : last + 1, :])
    direct = values * (step_wide * key_query + skip)
    gate_z = silu(dot32(normed[...], w_gate_z[...]))

    mark("state")

    def read_block(block, carry):
        rows = pl.ds(pl.multiple_of(block * 8, 8), 8)
        asked = queries[rows, :].astype(BF)
        row_of = lax.broadcasted_iota(jnp.int32, (8, width), 0)
        total_read = jnp.zeros((8, width), F32)
        for row in range(8):
            held = state[block * 8 + row].astype(BF)
            total_read = jnp.where(row_of == row, dot32_t(asked, held), total_read)
        state_read[rows, :] = total_read
        return carry

    for block in range(state_blocks):
        mark(f"statewait{block}")
        load_state(block).wait()
    mark("state")
    lax.fori_loop(0, seqs // 8, read_block, 0)

    mark("gated")
    gated = (decay_wide * state_read[...] + direct) * gate_z
    squared = gated * gated
    squared = jnp.concatenate(
        [squared[:, tile * LANES : (tile + 1) * LANES] for tile in range(tiles)], axis=0
    )
    head_sum = dot32(jnp.concatenate(halves(squared), axis=1), same_head)
    norm = lax.rsqrt(head_sum / HEAD_DIM + norm_epsilon)
    norm = jnp.concatenate(
        [norm[tile * seqs : (tile + 1) * seqs, :] for tile in range(tiles)], axis=1
    )
    mixed = (gated * norm * head_gain[...]).astype(BF)

    mark("outproj")
    load_out.wait()

    def mix_copy(step):
        return pltpu.make_async_remote_copy(
            src_ref=mix_send.at[step - 1],
            dst_ref=mix_recv.at[step - 1],
            send_sem=mix_send_sem,
            recv_sem=mix_recv_sem,
            device_id=(me_e, peer(step)),
            device_id_type=MESH,
        )

    def all_mixes():
        return pltpu.make_async_remote_copy(
            src_ref=mix_send,
            dst_ref=mix_recv,
            send_sem=mix_send_sem,
            recv_sem=mix_recv_sem,
            device_id=(me_e, peer(1)),
            device_id_type=MESH,
        )

    for step in steps:
        share = dot32(mixed, w_out[:, part_rows(step)])
        if step:
            mix_send[step - 1] = share.astype(BF)
            mix_copy(step).start()
        else:
            mix_sum = share
    mark("mixwait")
    all_mixes().wait_recv()
    mark("residual")
    for step in range(1, n_tp):
        mix_sum = mix_sum + mix_recv[step - 1].astype(F32)
    residual = (tokens[...].astype(F32) + mix_sum).astype(BF)

    def chunk(step):
        return pl.ds(step * n_ep, n_ep)

    def exchange(send, recv, send_sem, recv_sem, step, step_e):
        return pltpu.make_async_remote_copy(
            src_ref=send.at[step * n_ep + other_e(step_e)],
            dst_ref=recv.at[step * n_ep + me_e],
            send_sem=send_sem,
            recv_sem=recv_sem.at[step],
            device_id=(other_e(step_e), peer(step)),
            device_id_type=MESH,
        )

    def send_out(send, recv, send_sem, recv_sem, step):
        for step_e in far_first:
            if step or step_e:
                exchange(send, recv, send_sem, recv_sem, step, step_e).start()
        if step == 0:
            recv[me_e] = send[me_e]

    def await_chunk(send, recv, send_sem, recv_sem, step):
        blocks = chunk(step) if step else pl.ds(0, n_ep - 1)
        pltpu.make_async_remote_copy(
            src_ref=send.at[blocks],
            dst_ref=recv.at[blocks],
            send_sem=send_sem,
            recv_sem=recv_sem.at[step],
            device_id=(me_e, peer(1)),
            device_id_type=MESH,
        ).wait_recv()

    def await_sent(send, recv, send_sem, recv_sem):
        blocks = pl.ds(0, n_ep * n_tp - 1)
        pltpu.make_async_remote_copy(
            src_ref=send.at[blocks],
            dst_ref=recv.at[blocks],
            send_sem=send_sem,
            recv_sem=recv_sem.at[0],
            device_id=(me_e, peer(1)),
            device_id_type=MESH,
        ).wait_send()

    out_rows = (row_send, row_recv, row_send_sem, row_recv_sem)
    back_rows = (back_send, back_recv, back_send_sem, back_recv_sem)
    stack = jnp.concatenate(
        [residual[:, tile * LANES : (tile + 1) * LANES] for tile in range(tiles)], axis=0
    )
    for step in steps:
        mark(f"place{step}")
        outgoing = dot32(place[step], stack).astype(BF)
        row_send[chunk(step)] = outgoing.reshape(n_ep, lines, LANES)
        mark(f"rowsend{step}")
        send_out(*out_rows, step)

    mark("expwait")
    load_exp_gate.wait()
    load_exp_up.wait()
    load_exp_down.wait()
    pltpu.make_async_remote_copy(
        src_ref=gathered,
        dst_ref=gathered,
        send_sem=tok_send_sem,
        recv_sem=tok_recv_sem.at[0],
        device_id=(me_e, peer(1)),
        device_id_type=MESH,
    ).wait_send()
    all_mixes().wait_send()

    units = exp_gate.shape[1]
    squares = jnp.zeros((n_rows, 1), F32)
    for step in steps:
        mark(f"rowwait{step}")
        await_chunk(*out_rows, step)
        mark(f"gateup{step}")
        came = dot32(pick[...], row_recv[chunk(step)].reshape(n_lines, LANES))
        rows = part_rows(step)
        pieces = [came[tile * n_rows : (tile + 1) * n_rows, :] for tile in range(tiles)]
        for piece in pieces:
            squares = squares + jnp.sum(piece * piece, axis=1, keepdims=True)
        left = (jnp.concatenate(pieces, axis=1) * ffn_gain[:, rows]).astype(BF)
        scale = lax.rsqrt(squares / features + norm_epsilon)
        for at in range(units // TILE):
            columns = slice(at * TILE, (at + 1) * TILE)
            gate_part = dot32(left, exp_gate[rows, columns])
            up_part = dot32(left, exp_up[rows, columns])
            if step != steps[0]:
                gate_part = sum_egate[:, columns] + gate_part
                up_part = sum_eup[:, columns] + up_part
            if step != steps[-1]:
                sum_egate[:, columns] = gate_part
                sum_eup[:, columns] = up_part
            else:
                hidden[:, columns] = (silu(gate_part * scale) * (up_part * scale)).astype(BF)
    mark("down")

    def expert_part(step):
        result = dot32(hidden[...], exp_down[:, part_rows(step)]).astype(BF)
        return jnp.concatenate(
            [result[:, tile * LANES : (tile + 1) * LANES] for tile in range(tiles)], axis=0
        )

    part = expert_part(steps[0])
    for at, step in enumerate(steps):
        ready = part
        if at + 1 < n_tp:
            part = expert_part(steps[at + 1])
        back_send[chunk(step)] = dot32(unpick[...], ready).astype(BF).reshape(n_ep, lines, LANES)
        send_out(*back_rows, step)
    mark("rowdrain")
    await_sent(*out_rows)
    moe_sum = jnp.zeros((tiles * seqs, LANES), F32)
    for step in range(n_tp):
        mark(f"backwait{step}")
        await_chunk(*back_rows, step)
        mark(f"combine{step}")
        came = back_recv[chunk(step)].reshape(n_lines, LANES)
        moe_sum = moe_sum + dot32(comb_high[step], came) + dot32(comb_low[step], came)
    for tile in range(tiles):
        columns = slice(tile * LANES, (tile + 1) * LANES)
        part = moe_sum[tile * seqs : (tile + 1) * seqs, :]
        out[:, columns] = (residual[:, columns].astype(F32) + part).astype(BF)
    mark("drain")
    await_sent(*back_rows)
    mark(None)


def local(
    tokens,
    mix_gain,
    w_gate_z,
    w_value_x,
    w_key_b,
    w_query_c,
    w_step,
    step_bias,
    decay_log,
    skip_gain,
    conv_x_weight,
    conv_b_weight,
    conv_c_weight,
    window_x,
    window_b,
    window_c,
    ssm_state,
    head_gain,
    w_out,
    ffn_gain,
    route_ids,
    route_weights,
    expert_gate,
    expert_up,
    expert_down,
):
    n_ep, n_tp = lax.axis_size("ep"), lax.axis_size("tp")
    seqs, width = tokens.shape
    features = width * n_tp
    units = expert_gate.shape[2]
    slots = -(-3 * seqs * route_ids.shape[1] // (2 * EXP_IN * n_ep))
    while slots * (width // LANES) % 8:
        slots = slots + 1
    if (
        n_tp != EXP_IN
        or n_tp != 4
        or route_ids.shape[1] != 2
        or width % LANES
        or units % TILE
        or seqs % 16
        or n_ep * slots % 16
        or n_ep * EXP_IN > 256
    ):
        return local_plain(
            tokens, mix_gain, w_gate_z, w_value_x, w_key_b, w_query_c, w_step, step_bias,
            decay_log, skip_gain, conv_x_weight, conv_b_weight, conv_c_weight, window_x,
            window_b, window_c, ssm_state, head_gain, w_out, ffn_gain, route_ids,
            route_weights, expert_gate, expert_up, expert_down,
        )
    state_rows = ssm_state.reshape(seqs, width, STATE)
    small = [
        tokens,
        mix_gain[None],
        step_bias[None],
        decay_log[None],
        skip_gain[None],
        conv_x_weight,
        conv_b_weight,
        conv_c_weight,
        window_x.transpose(1, 0, 2),
        window_b.transpose(1, 0, 2),
        window_c.transpose(1, 0, 2),
        head_gain[None],
        ffn_gain[None],
        route_ids.T,
        route_weights.T,
    ]
    large = [
        w_gate_z, w_value_x, w_key_b, w_query_c, w_step.T, state_rows, w_out,
        expert_gate[0], expert_up[0], expert_down[0],
    ]
    operands = [pltpu.with_memory_space_constraint(each, pltpu.HBM) for each in small + large]
    tiles = width // LANES
    n_rows = n_ep * slots
    n_lines = n_rows * tiles
    exchange = (n_ep * n_tp, tiles * slots, LANES)
    vmem = pltpu.VMEM
    dma = pltpu.SemaphoreType.DMA
    return pl.pallas_call(
        functools.partial(layer_entry, n_ep, n_tp, slots, len(small)),
        out_shape=pltpu.VMEM((seqs, width), BF),
        in_specs=[pl.BlockSpec(memory_space=pl.ANY)] * len(operands),
        out_specs=pl.BlockSpec(memory_space=pltpu.VMEM),
        scratch_shapes=[
            vmem(w_gate_z.shape, BF),
            vmem(w_value_x.shape, BF),
            vmem((features, STATE), BF),
            vmem((features, STATE), BF),
            vmem(w_step.shape[::-1], BF),
            vmem(state_rows.shape, F32),
            vmem(w_out.shape, BF),
            vmem(expert_gate.shape[1:], BF),
            vmem(expert_up.shape[1:], BF),
            vmem(expert_down.shape[1:], BF),
            vmem((n_tp - 1, seqs, width), BF),
            vmem((seqs, features), BF),
            vmem((seqs, STATE), F32),
            vmem((seqs, width), F32),
            vmem((n_tp - 1, seqs, width), BF),
            vmem((n_tp - 1, seqs, width), BF),
            vmem(exchange, BF),
            vmem(exchange, BF),
            vmem((n_tp, n_lines, tiles * seqs), BF),
            vmem((n_tp, tiles * seqs, n_lines), BF),
            vmem((n_tp, tiles * seqs, n_lines), BF),
            vmem((n_lines, n_lines), BF),
            vmem((n_lines, n_lines), BF),
            vmem((n_rows, units), F32),
            vmem((n_rows, units), F32),
            vmem((n_rows, units), BF),
            vmem(exchange, BF),
            vmem(exchange, BF),
            dma((9,)),
            dma((2,)),
            dma,
            dma((n_tp - 1,)),
            dma,
            dma,
            dma,
            dma((n_tp,)),
            dma,
            dma((n_tp,)),
            *[vmem(each.shape, each.dtype) for each in small],
            dma((len(small),)),
        ],
        compiler_params=pltpu.CompilerParams(
            collective_id=0, has_side_effects=True, vmem_limit_bytes=60 * 1024 * 1024
        ),
        name="layer",
    )(*operands)


def solution(mesh):
    in_specs = (
        P("ep", "tp"),
        P(),
        P(None, "tp"),
        P(None, "tp"),
        P(),
        P(),
        P(),
        P(),
        P(),
        P(),
        P(None, "tp"),
        P(),
        P(),
        P("ep", None, "tp"),
        P("ep", None, None),
        P("ep", None, None),
        P("ep", "tp", None, None),
        P("tp"),
        P("tp", None),
        P(),
        P("ep", None),
        P("ep", None),
        P("ep", None, "tp"),
        P("ep", None, "tp"),
        P("ep", "tp", None),
    )
    out_specs = P("ep", "tp")
    return jax.shard_map(local, mesh=mesh, in_specs=in_specs, out_specs=out_specs, check_vma=False)
```

```python
import functools

import jax
import jax.numpy as jnp
from jax import lax
from jax.experimental import pallas as pl
from jax.experimental.pallas import tpu as pltpu
from jax.sharding import PartitionSpec as P

HEADS = 32
HEAD_DIM = 64
STATE = 128
GROUPS = 2
EXP_IN = 4


norm_epsilon = 1e-06


def row_norm(arr_values, norm_gain):
    widened = arr_values.astype(jnp.float32)
    return (
        widened
        * lax.rsqrt(jnp.mean(widened * widened, axis=-1, keepdims=True) + norm_epsilon)
        * norm_gain
    )


def short_conv(window, fresh_row, weight):
    conv_taps = weight.astype(jnp.float32)
    summed = (
        jnp.sum(window.astype(jnp.float32) * conv_taps[:-1][None], axis=1)
        + fresh_row * conv_taps[-1]
    )
    return jax.nn.silu(summed)


def product(left, right):
    return jnp.dot(left, right, preferred_element_type=jnp.float32)


def local_plain(
    tokens,
    mix_gain,
    w_gate_z,
    w_value_x,
    w_key_b,
    w_query_c,
    w_step,
    step_bias,
    decay_log,
    skip_gain,
    conv_x_weight,
    conv_b_weight,
    conv_c_weight,
    window_x,
    window_b,
    window_c,
    ssm_state,
    head_gain,
    w_out,
    ffn_gain,
    route_ids,
    route_weights,
    expert_gate,
    expert_up,
    expert_down,
):
    tp_index = lax.axis_index("tp")
    tp_count = lax.axis_size("tp")
    ep_count = lax.axis_size("ep")
    seq_count = tokens.shape[0]
    gathered = lax.all_gather(tokens, "tp", axis=1, tiled=True)
    normed = row_norm(gathered, mix_gain).astype(jnp.bfloat16)
    local_width = w_gate_z.shape[1]
    head_count = local_width // HEAD_DIM
    first_head = tp_index * head_count
    group_start = first_head // (HEADS // GROUPS) * STATE
    gate_z = product(normed, w_gate_z)
    values = short_conv(window_x, product(normed, w_value_x), conv_x_weight)
    key_b = short_conv(
        lax.dynamic_slice_in_dim(window_b, group_start, STATE, 2),
        product(normed, lax.dynamic_slice_in_dim(w_key_b, group_start, STATE, 1)),
        lax.dynamic_slice_in_dim(conv_b_weight, group_start, STATE, 1),
    )
    query_c = short_conv(
        lax.dynamic_slice_in_dim(window_c, group_start, STATE, 2),
        product(normed, lax.dynamic_slice_in_dim(w_query_c, group_start, STATE, 1)),
        lax.dynamic_slice_in_dim(conv_c_weight, group_start, STATE, 1),
    )
    step_all = product(normed, w_step) + step_bias
    step_size = jax.nn.softplus(lax.dynamic_slice_in_dim(step_all, first_head, head_count, 1))
    rate_heads = jnp.exp(lax.dynamic_slice_in_dim(decay_log, first_head, head_count, 0))
    skip_heads = lax.dynamic_slice_in_dim(skip_gain, first_head, head_count, 0)
    decay_heads = jnp.exp(-step_size * rate_heads)
    value_heads = values.reshape(seq_count, head_count, HEAD_DIM)
    new_state = (
        decay_heads[:, :, None, None] * ssm_state
        + (step_size[:, :, None] * value_heads)[..., None] * key_b[:, None, None, :]
    )
    read_out = jnp.einsum("shpn,sn->shp", new_state, query_c, precision=lax.Precision.HIGHEST)
    read_out = read_out + skip_heads[None, :, None] * value_heads
    gated = read_out * jax.nn.silu(gate_z.reshape(seq_count, head_count, HEAD_DIM))
    gated = gated * lax.rsqrt(jnp.mean(gated * gated, axis=-1, keepdims=True) + norm_epsilon)
    mixed_heads = (
        (gated * head_gain.reshape(head_count, HEAD_DIM))
        .reshape(seq_count, local_width)
        .astype(jnp.bfloat16)
    )
    partial_value = product(mixed_heads, w_out)
    share_mix = lax.psum_scatter(partial_value, "tp", scatter_dimension=1, tiled=True)
    residual_own = (tokens.astype(jnp.float32) + share_mix).astype(jnp.bfloat16)
    residual_full = lax.all_gather(residual_own, "tp", axis=1, tiled=True)
    ffn_in = row_norm(residual_full, ffn_gain).astype(jnp.bfloat16)
    top_count = route_ids.shape[1]
    expert_count = EXP_IN * ep_count
    capacity = max(2, (3 * seq_count * top_count + 2 * expert_count - 1) // (2 * expert_count))
    sub_index = tp_index // (tp_count // EXP_IN)
    target_set = route_ids // EXP_IN
    hit_mask = route_ids % EXP_IN == sub_index
    set_grid = jnp.arange(ep_count, dtype=jnp.int32)
    set_onehot = (hit_mask[:, :, None] & (target_set[:, :, None] == set_grid)).astype(jnp.int32)
    set_onehot = set_onehot.reshape(seq_count * top_count, ep_count)
    earlier = jnp.cumsum(set_onehot, axis=0) - set_onehot
    slot_rank = jnp.sum(earlier * set_onehot, axis=1).reshape(seq_count, top_count)
    slot_index = jnp.where(hit_mask, target_set * capacity + slot_rank, -1)
    slot_grid = jnp.arange(ep_count * capacity, dtype=jnp.int32)
    slot_match = slot_index[:, :, None] == slot_grid
    placed = jnp.any(slot_match, axis=1).astype(jnp.bfloat16)
    outgoing = jnp.einsum("sj,sd->jd", placed, ffn_in, preferred_element_type=jnp.float32)
    outgoing = outgoing.astype(jnp.bfloat16).reshape(ep_count, capacity, ffn_in.shape[1])
    route_share = route_weights / jnp.sum(route_weights, axis=1, keepdims=True)
    combine_weight = jnp.sum(jnp.where(slot_match, route_share[:, :, None], 0.0), axis=1)
    arrived = lax.all_to_all(outgoing, "ep", split_axis=0, concat_axis=0, tiled=True)
    source_count, slot_count, row_width = arrived.shape
    flat_rows = arrived.reshape(source_count * slot_count, row_width)
    gate_part = product(flat_rows, expert_gate[0])
    up_part = product(flat_rows, expert_up[0])
    hidden = (jax.nn.silu(gate_part) * up_part).astype(jnp.bfloat16)
    expert_out = product(hidden, expert_down[0]).reshape(source_count, slot_count, row_width)
    returned = lax.all_to_all(
        expert_out.astype(jnp.bfloat16), "ep", split_axis=0, concat_axis=0, tiled=True
    ).astype(expert_out.dtype)
    moe_part = jnp.dot(
        combine_weight,
        returned.reshape(ep_count * capacity, -1),
        precision=lax.Precision.HIGHEST,
        preferred_element_type=jnp.float32,
    )
    moe_share = lax.psum_scatter(
        moe_part.astype(jnp.bfloat16), "tp", scatter_dimension=1, tiled=True
    ).astype(jnp.float32)
    return (residual_own.astype(jnp.float32) + moe_share).astype(jnp.bfloat16)


MESH = pl.DeviceIdType.MESH
HIGH = lax.Precision.HIGHEST
BF = jnp.bfloat16
F32 = jnp.float32
LANES = 128
TILE = 256
ROW_SEND, ROW_USE = (0, 1, 2, 3), (0, 1, 2, 3)


def silu(v):
    return v / (1.0 + jnp.exp(-v))


def dot32(left, right, precision=None):
    return jnp.dot(left, right, preferred_element_type=F32, precision=precision)


def dot32_t(left, right):
    return lax.dot_general(left, right, (((1,), (1,)), ((), ())), preferred_element_type=F32)


def halves(v):
    high = v.astype(BF)
    return high, (v - high.astype(F32)).astype(BF)


def split_index(index, *counts):
    digits = []
    for place in range(len(counts) - 1):
        below = 1
        for count in counts[place + 1 :]:
            below = below * count
        digit = jnp.zeros_like(index)
        for step in range(1, counts[place]):
            digit = digit + jnp.where(index >= step * below, 1, 0)
        index = index - digit * below
        digits.append(digit)
    return (*digits, index)


_open = []


def mark(name):
    if _open:
        _open.pop().__exit__(None, None, None)
    if name:
        scope = jax.named_scope(name)
        scope.__enter__()
        _open.append(scope)


def layer_entry(n_ep, n_tp, slots, n_small, *refs):
    held, small_sem = refs[-1 - n_small : -1], refs[-1]
    fetches = [
        pltpu.make_async_copy(refs[at], held[at], small_sem.at[at]) for at in range(n_small)
    ]
    layer_kernel(n_ep, n_tp, slots, fetches, *held, *refs[n_small : -1 - n_small])


def layer_kernel(
    n_ep,
    n_tp,
    slots,
    fetches,
    tokens,
    mix_gain,
    step_bias,
    decay_log,
    skip_gain,
    conv_x,
    conv_b,
    conv_c,
    window_x,
    window_b,
    window_c,
    head_gain,
    ffn_gain,
    ids_t,
    scores_t,
    hbm_gate_z,
    hbm_value_x,
    hbm_key_b,
    hbm_query_c,
    hbm_step,
    hbm_state,
    hbm_out,
    hbm_exp_gate,
    hbm_exp_up,
    hbm_exp_down,
    out,
    w_gate_z,
    w_value_x,
    w_key_b,
    w_query_c,
    w_step,
    state,
    w_out,
    exp_gate,
    exp_up,
    exp_down,
    gathered,
    normed,
    queries,
    state_read,
    mix_send,
    mix_recv,
    row_send,
    row_recv,
    place,
    comb_high,
    comb_low,
    pick,
    unpick,
    sum_egate,
    sum_eup,
    hidden,
    back_send,
    back_recv,
    load_sem,
    state_sem,
    tok_send_sem,
    tok_recv_sem,
    mix_send_sem,
    mix_recv_sem,
    row_send_sem,
    row_recv_sem,
    back_send_sem,
    back_recv_sem,
    chain_sem,
):
    me_e = lax.axis_index("ep")
    me_t = lax.axis_index("tp")
    seqs, width = tokens.shape
    features = width * n_tp
    tiles = width // LANES
    n_lines = n_ep * slots * tiles
    n_rows = hidden.shape[0]
    carried = (n_ep, slots, tiles, LANES)
    heads_here = width // HEAD_DIM
    first_head = me_t * heads_here
    group_start = pl.multiple_of(first_head // (HEADS // GROUPS) * STATE, STATE)
    group_cols = pl.ds(group_start, STATE)
    state_blocks = state_sem.shape[0]
    state_rows = seqs // state_blocks

    def peer(step):
        row, column = me_t // 2, lax.rem(me_t, 2)
        return lax.rem(row + step // 2, 2) * 2 + lax.rem(column + step % 2, 2)

    def other_e(step):
        return lax.rem(me_e + step, n_ep)

    far_first = sorted(range(n_ep), key=lambda step: -min(step, n_ep - step))
    steps = tuple(reversed(range(n_tp)))

    def load(source, target, index):
        return pltpu.make_async_copy(source, target, load_sem.at[index])

    load_key = load(hbm_key_b.at[:, group_cols], w_key_b, 0)
    load_query = load(hbm_query_c.at[:, group_cols], w_query_c, 1)
    load_step = load(hbm_step, w_step, 2)
    load_value = load(hbm_value_x, w_value_x, 3)
    load_gate = load(hbm_gate_z, w_gate_z, 4)
    load_out = load(hbm_out, w_out, 5)
    load_exp_gate = load(hbm_exp_gate, exp_gate, 6)
    load_exp_up = load(hbm_exp_up, exp_up, 7)
    load_exp_down = load(hbm_exp_down, exp_down, 8)

    def load_state(block):
        rows = pl.ds(block * state_rows, state_rows)
        return pltpu.make_async_copy(hbm_state.at[rows], state.at[rows], state_sem.at[block])

    mark("greet")
    for each in fetches:
        each.start()
    barrier = pltpu.get_barrier_semaphore()
    for step in range(1, n_tp):
        pl.semaphore_signal(
            barrier, inc=1, device_id=(me_e, peer(step)), device_id_type=MESH
        )
    partner = me_e // 2 * 2 + 1 - lax.rem(me_e, 2)
    has_below = (me_e + n_ep - 2) // n_ep
    has_above = (2 * n_ep - 3 - me_e) // n_ep

    def signal_e(semaphore, to_e):
        pl.semaphore_signal(semaphore, inc=1, device_id=(to_e, me_t), device_id_type=MESH)

    signal_e(barrier, partner)

    @pl.when(has_below == 1)
    def _():
        signal_e(barrier, me_e - 2)

    @pl.when(has_above == 1)
    def _():
        signal_e(barrier, me_e + 2)

    def chain_send(turn):
        @pl.when(has_below == 1)
        def _():
            signal_e(chain_sem.at[turn, 0], me_e - 2)

        @pl.when(has_above == 1)
        def _():
            signal_e(chain_sem.at[turn, 1], me_e + 2)

    def chain_wait(turn):
        @pl.when(has_above == 1)
        def _():
            pl.semaphore_wait(chain_sem.at[turn, 0], 1)

        @pl.when(has_below == 1)
        def _():
            pl.semaphore_wait(chain_sem.at[turn, 1], 1)

    turns = n_ep // 2 - 1

    def turn_on(start, stop):
        for turn in range(start, stop):
            if turn < turns:
                chain_wait(turn - 1)
                chain_send(turn)

    mark("loads")
    for each in (load_query, load_key, load_step, load_value, load_gate):
        each.start()
    for block in range(state_blocks):
        load_state(block).start(priority=1)
    mark("smallwait")
    fetches[0].wait()
    mark("barrier")
    pl.semaphore_wait(barrier, n_tp + has_below + has_above)
    mark("toksend")

    def token_copy(step):
        return pltpu.make_async_remote_copy(
            src_ref=tokens,
            dst_ref=gathered.at[step - 1],
            send_sem=tok_send_sem,
            recv_sem=tok_recv_sem.at[step - 1],
            device_id=(me_e, peer(step)),
            device_id_type=MESH,
        )

    for step in reversed(range(1, n_tp)):
        token_copy(step).start()
    chain_send(0)
    mark("smallrest")
    for each in fetches[1:]:
        each.wait()

    def part_rows(step):
        return pl.ds(pl.multiple_of(peer(step) * width, width), width)

    def squares_of(piece):
        wide = piece.astype(F32)
        return jnp.sum(wide * wide, axis=1, keepdims=True)

    mark("routes")
    n_exp = n_ep * EXP_IN
    row_at = lax.broadcasted_iota(jnp.int32, (seqs, seqs), 0)
    col_at = lax.broadcasted_iota(jnp.int32, (seqs, seqs), 1)

    def stood_up(row):
        return jnp.sum(jnp.where(row_at == col_at, row, 0.0), axis=1, keepdims=True)

    id0 = stood_up(ids_t[0:1, :].astype(F32)).astype(jnp.int32)
    id1 = stood_up(ids_t[1:2, :].astype(F32)).astype(jnp.int32)
    lane_exp = lax.broadcasted_iota(jnp.int32, (seqs, n_exp), 1)
    hit0 = jnp.where(id0 == lane_exp, 1.0, 0.0)
    hit1 = jnp.where(id1 == lane_exp, 1.0, 0.0)
    lower = jnp.where(row_at > col_at, 1.0, 0.0).astype(BF)
    upper = jnp.where(row_at < col_at, 1.0, 0.0).astype(BF)
    before = dot32(lower, (hit0 + hit1).astype(BF))
    slot0 = id0 * slots + jnp.sum(before * hit0, axis=1, keepdims=True).astype(jnp.int32)
    slot1 = id1 * slots + jnp.sum(before * hit1, axis=1, keepdims=True).astype(jnp.int32)
    score0, score1 = stood_up(scores_t[0:1, :]), stood_up(scores_t[1:2, :])
    total = score0 + score1

    def stacked(column):
        return jnp.concatenate([column] * tiles, axis=0)

    slot0, slot1 = stacked(slot0), stacked(slot1)
    share0, share1 = stacked(score0 / total), stacked(score1 / total)

    idt0, idt1 = ids_t[0:1, :], ids_t[1:2, :]
    sub_exp = lax.broadcasted_iota(jnp.int32, (n_exp, seqs), 0)
    hitt0 = jnp.where(idt0 == sub_exp, 1.0, 0.0)
    hitt1 = jnp.where(idt1 == sub_exp, 1.0, 0.0)
    before_t = dot32((hitt0 + hitt1).astype(BF), upper)
    rank0 = jnp.sum(before_t * hitt0, axis=0, keepdims=True)
    rank1 = jnp.sum(before_t * hitt1, axis=0, keepdims=True)
    rep_row = lax.broadcasted_iota(jnp.int32, (seqs, tiles * seqs), 0)
    rep_col = lax.broadcasted_iota(jnp.int32, (1, tiles * seqs), 1)
    tile_col, token_col = split_index(rep_col, tiles, seqs)
    repeat = jnp.where(rep_row == token_col, 1.0, 0.0).astype(BF)
    wide_ids = dot32(
        jnp.concatenate([idt0.astype(F32), idt1.astype(F32), rank0, rank1] * 2, axis=0).astype(BF),
        repeat,
    ).astype(jnp.int32)
    slott0 = wide_ids[0:1, :] * slots + wide_ids[2:3, :]
    slott1 = wide_ids[1:2, :] * slots + wide_ids[3:4, :]

    line_row = lax.broadcasted_iota(jnp.int32, (n_lines, 1), 0)
    e_row, k_row, c_row = split_index(line_row, n_ep, slots, tiles)
    line_col = lax.broadcasted_iota(jnp.int32, (1, n_lines), 1)
    e_col, k_col, c_col = split_index(line_col, n_ep, slots, tiles)
    tok_row = lax.broadcasted_iota(jnp.int32, (tiles * seqs, 1), 0)
    tile_row, _ = split_index(tok_row, tiles, seqs)
    pick_row = lax.broadcasted_iota(jnp.int32, (tiles * n_rows, 1), 0)
    pick[...] = jnp.where(
        pick_row == c_col * n_rows + e_col * slots + k_col, 1.0, 0.0
    ).astype(BF)
    pick_col = lax.broadcasted_iota(jnp.int32, (1, tiles * n_rows), 1)
    unpick[...] = jnp.where(
        pick_col == c_row * n_rows + e_row * slots + k_row, 1.0, 0.0
    ).astype(BF)
    for step in range(n_tp):
        there_row = (e_row * n_tp + peer(step)) * slots + k_row
        there_col = (e_col * n_tp + peer(step)) * slots + k_col
        same = c_row == tile_col
        chosen = same & ((slott0 == there_row) | (slott1 == there_row))
        place[step] = jnp.where(chosen, 1.0, 0.0).astype(BF)
        same = tile_row == c_col
        weight = jnp.where(same & (slot0 == there_col), share0, 0.0) + jnp.where(
            same & (slot1 == there_col), share1, 0.0
        )
        comb_high[step], comb_low[step] = halves(weight)

    mark("pasts")

    def window_sum(window, taps, columns):
        summed = None
        for tap in range(window.shape[0]):
            term = window[tap, :, columns].astype(F32) * taps[tap : tap + 1, :]
            summed = term if summed is None else summed + term
        return summed

    every = pl.ds(0, width)
    taps_x = conv_x[...].astype(F32)
    taps_b = conv_b[:, group_cols].astype(F32)
    taps_c = conv_c[:, group_cols].astype(F32)
    last = taps_x.shape[0] - 1
    past_x = window_sum(window_x, taps_x, every)
    past_b = window_sum(window_b, taps_b, group_cols)
    past_c = window_sum(window_c, taps_c, group_cols)
    head_row = lax.broadcasted_iota(jnp.int32, (HEADS, width), 0)
    head_col = lax.broadcasted_iota(jnp.int32, (HEADS, width), 1) // HEAD_DIM + first_head
    spread = jnp.where(head_row == head_col, 1.0, 0.0).astype(BF)
    same_row = lax.rem(lax.broadcasted_iota(jnp.int32, (2 * LANES, LANES), 0), LANES) // HEAD_DIM
    same_col = lax.broadcasted_iota(jnp.int32, (2 * LANES, LANES), 1) // HEAD_DIM
    same_head = jnp.where(same_row == same_col, 1.0, 0.0).astype(BF)
    skip = dot32(jnp.broadcast_to(skip_gain[...], (8, HEADS)), spread.astype(F32), HIGH)[0:1, :]

    squares = squares_of(tokens[...])
    for step in range(1, n_tp):
        mark(f"tokwait{step}")
        token_copy(step).wait_recv()
        squares = squares + squares_of(gathered[step - 1])
    mark("norm")
    for each in (load_out, load_exp_gate, load_exp_up, load_exp_down):
        each.start(priority=1)
    scale = lax.rsqrt(squares / features + norm_epsilon)
    for step in range(n_tp):
        piece = gathered[step - 1] if step else tokens[...]
        columns = part_rows(step)
        normed[:, columns] = (piece.astype(F32) * scale * mix_gain[:, columns]).astype(BF)
    turn_on(1, 2)
    mark("projwait")
    for each in (load_query, load_key, load_step, load_value, load_gate):
        each.wait()
    mark("query")
    query = silu(past_c + dot32(normed[...], w_query_c[...]) * taps_c[last : last + 1, :])
    key = silu(past_b + dot32(normed[...], w_key_b[...]) * taps_b[last : last + 1, :])
    key_query = jnp.sum(key * query, axis=1, keepdims=True)
    raw_step = dot32_t(normed[...], w_step[...]) + step_bias[...]
    step_size = jnp.maximum(raw_step, 0.0) + jnp.log1p(jnp.exp(-jnp.abs(raw_step)))
    decay = jnp.exp(-step_size * jnp.exp(decay_log[...]))
    spread_high, spread_low = halves(jnp.concatenate([step_size, decay], axis=0))
    wide = dot32(jnp.concatenate([spread_high, spread_low], axis=0), spread)
    step_wide = wide[0:seqs] + wide[2 * seqs : 3 * seqs]
    decay_wide = wide[seqs : 2 * seqs] + wide[3 * seqs : 4 * seqs]
    mark("value")
    values = silu(past_x + dot32(normed[...], w_value_x[...]) * taps_x[last : last + 1, :])
    direct = values * (step_wide * key_query + skip)
    gate_z = silu(dot32(normed[...], w_gate_z[...]))

    mark("state")

    queries[...] = query
    turn_on(2, turns)

    def read_block(block, carry):
        load_state(block).wait()
        rows = pl.ds(pl.multiple_of(block * 8, 8), 8)
        asked = queries[rows, :].astype(BF)
        row_of = lax.broadcasted_iota(jnp.int32, (8, width), 0)
        total_read = jnp.zeros((8, width), F32)
        for row in range(8):
            held = state[block * 8 + row].astype(BF)
            total_read = jnp.where(row_of == row, dot32_t(asked, held), total_read)
        state_read[rows, :] = total_read
        return carry

    lax.fori_loop(0, seqs // 8, read_block, 0)
    mark("gated")
    gated = (decay_wide * state_read[...] + direct) * gate_z
    squared = gated * gated
    squared = jnp.concatenate(
        [squared[:, tile * LANES : (tile + 1) * LANES] for tile in range(tiles)], axis=0
    )
    head_sum = dot32(jnp.concatenate(halves(squared), axis=1), same_head)
    norm = lax.rsqrt(head_sum / HEAD_DIM + norm_epsilon)
    norm = jnp.concatenate(
        [norm[tile * seqs : (tile + 1) * seqs, :] for tile in range(tiles)], axis=1
    )
    mixed = (gated * norm * head_gain[...]).astype(BF)

    mark("outproj")
    chain_wait(turns - 1)
    load_out.wait()

    def mix_copy(step):
        return pltpu.make_async_remote_copy(
            src_ref=mix_send.at[step - 1],
            dst_ref=mix_recv.at[step - 1],
            send_sem=mix_send_sem,
            recv_sem=mix_recv_sem,
            device_id=(me_e, peer(step)),
            device_id_type=MESH,
        )

    def all_mixes():
        return pltpu.make_async_remote_copy(
            src_ref=mix_send,
            dst_ref=mix_recv,
            send_sem=mix_send_sem,
            recv_sem=mix_recv_sem,
            device_id=(me_e, peer(1)),
            device_id_type=MESH,
        )

    for step in steps:
        share = dot32(mixed, w_out[:, part_rows(step)])
        if step:
            mix_send[step - 1] = share.astype(BF)
            mix_copy(step).start()
        else:
            mix_sum = share
    mark("mixwait")
    all_mixes().wait_recv()
    mark("residual")
    for step in range(1, n_tp):
        mix_sum = mix_sum + mix_recv[step - 1].astype(F32)
    residual = (tokens[...].astype(F32) + mix_sum).astype(BF)

    def chunk(step):
        return pl.ds(step * n_ep, n_ep)

    def exchange(send, recv, send_sem, recv_sem, step, step_e):
        return pltpu.make_async_remote_copy(
            src_ref=send.at[step * n_ep + other_e(step_e)],
            dst_ref=recv.at[step * n_ep + me_e],
            send_sem=send_sem,
            recv_sem=recv_sem.at[step],
            device_id=(other_e(step_e), peer(step)),
            device_id_type=MESH,
        )

    def send_out(send, recv, send_sem, recv_sem, step):
        for step_e in far_first:
            if step or step_e:
                exchange(send, recv, send_sem, recv_sem, step, step_e).start()
        if step == 0:
            recv[me_e] = send[me_e]

    def await_chunk(send, recv, send_sem, recv_sem, step):
        blocks = chunk(step) if step else pl.ds(0, n_ep - 1)
        pltpu.make_async_remote_copy(
            src_ref=send.at[blocks],
            dst_ref=recv.at[blocks],
            send_sem=send_sem,
            recv_sem=recv_sem.at[step],
            device_id=(me_e, peer(1)),
            device_id_type=MESH,
        ).wait_recv()

    def await_sent(send, recv, send_sem, recv_sem):
        blocks = pl.ds(0, n_ep * n_tp - 1)
        pltpu.make_async_remote_copy(
            src_ref=send.at[blocks],
            dst_ref=recv.at[blocks],
            send_sem=send_sem,
            recv_sem=recv_sem.at[0],
            device_id=(me_e, peer(1)),
            device_id_type=MESH,
        ).wait_send()

    out_rows = (row_send, row_recv, row_send_sem, row_recv_sem)
    back_rows = (back_send, back_recv, back_send_sem, back_recv_sem)
    stack = jnp.concatenate(
        [residual[:, tile * LANES : (tile + 1) * LANES] for tile in range(tiles)], axis=0
    )
    for step in ROW_SEND:
        mark(f"place{step}")
        outgoing = dot32(place[step], stack).astype(BF)
        row_send[chunk(step)] = outgoing.reshape(carried)
        mark(f"rowsend{step}")
        send_out(*out_rows, step)

    mark("expwait")
    load_exp_gate.wait()
    load_exp_up.wait()
    load_exp_down.wait()
    pltpu.make_async_remote_copy(
        src_ref=gathered,
        dst_ref=gathered,
        send_sem=tok_send_sem,
        recv_sem=tok_recv_sem.at[0],
        device_id=(me_e, peer(1)),
        device_id_type=MESH,
    ).wait_send()
    all_mixes().wait_send()

    units = exp_gate.shape[1]
    squares = jnp.zeros((n_rows, 1), F32)
    for step in ROW_USE:
        mark(f"rowwait{step}")
        await_chunk(*out_rows, step)
        mark(f"gateup{step}")
        came = dot32(pick[...], row_recv[chunk(step)].reshape(n_lines, LANES))
        rows = part_rows(step)
        pieces = [came[tile * n_rows : (tile + 1) * n_rows, :] for tile in range(tiles)]
        for piece in pieces:
            squares = squares + jnp.sum(piece * piece, axis=1, keepdims=True)
        left = (jnp.concatenate(pieces, axis=1) * ffn_gain[:, rows]).astype(BF)
        scale = lax.rsqrt(squares / features + norm_epsilon)
        for at in range(units // TILE):
            columns = slice(at * TILE, (at + 1) * TILE)
            gate_part = dot32(left, exp_gate[rows, columns])
            up_part = dot32(left, exp_up[rows, columns])
            if step != ROW_USE[0]:
                gate_part = sum_egate[:, columns] + gate_part
                up_part = sum_eup[:, columns] + up_part
            if step != ROW_USE[-1]:
                sum_egate[:, columns] = gate_part
                sum_eup[:, columns] = up_part
            else:
                hidden[:, columns] = (silu(gate_part * scale) * (up_part * scale)).astype(BF)
    mark("down")

    def expert_part(step):
        result = dot32(hidden[...], exp_down[:, part_rows(step)])
        return jnp.concatenate(
            [result[:, tile * LANES : (tile + 1) * LANES] for tile in range(tiles)], axis=0
        ).astype(BF)

    part = expert_part(steps[0])
    for at, step in enumerate(steps):
        ready = part
        if at + 1 < n_tp:
            part = expert_part(steps[at + 1])
        back_send[chunk(step)] = dot32(unpick[...], ready).astype(BF).reshape(carried)
        send_out(*back_rows, step)
    mark("rowdrain")
    await_sent(*out_rows)
    moe_sum = jnp.zeros((tiles * seqs, LANES), F32)
    for step in steps:
        mark(f"backwait{step}")
        await_chunk(*back_rows, step)
        mark(f"combine{step}")
        came = back_recv[chunk(step)].reshape(n_lines, LANES)
        moe_sum = moe_sum + dot32(comb_high[step], came) + dot32(comb_low[step], came)
    for tile in range(tiles):
        columns = slice(tile * LANES, (tile + 1) * LANES)
        part = moe_sum[tile * seqs : (tile + 1) * seqs, :]
        out[:, columns] = (residual[:, columns].astype(F32) + part).astype(BF)
    mark("drain")
    await_sent(*back_rows)
    mark(None)


def local(
    tokens,
    mix_gain,
    w_gate_z,
    w_value_x,
    w_key_b,
    w_query_c,
    w_step,
    step_bias,
    decay_log,
    skip_gain,
    conv_x_weight,
    conv_b_weight,
    conv_c_weight,
    window_x,
    window_b,
    window_c,
    ssm_state,
    head_gain,
    w_out,
    ffn_gain,
    route_ids,
    route_weights,
    expert_gate,
    expert_up,
    expert_down,
):
    n_ep, n_tp = lax.axis_size("ep"), lax.axis_size("tp")
    seqs, width = tokens.shape
    features = width * n_tp
    units = expert_gate.shape[2]
    slots = -(-3 * seqs * route_ids.shape[1] // (2 * EXP_IN * n_ep))
    if (
        n_tp != EXP_IN
        or n_tp != 4
        or route_ids.shape[1] != 2
        or width % LANES
        or units % TILE
        or seqs % 16
        or n_ep * slots * (width // LANES) % 16
        or n_ep % 2
        or n_ep < 4
        or n_ep * EXP_IN > 256
    ):
        return local_plain(
            tokens, mix_gain, w_gate_z, w_value_x, w_key_b, w_query_c, w_step, step_bias,
            decay_log, skip_gain, conv_x_weight, conv_b_weight, conv_c_weight, window_x,
            window_b, window_c, ssm_state, head_gain, w_out, ffn_gain, route_ids,
            route_weights, expert_gate, expert_up, expert_down,
        )
    state_rows = ssm_state.reshape(seqs, width, STATE)
    small = [
        tokens,
        mix_gain[None],
        step_bias[None],
        decay_log[None],
        skip_gain[None],
        conv_x_weight,
        conv_b_weight,
        conv_c_weight,
        window_x.transpose(1, 0, 2),
        window_b.transpose(1, 0, 2),
        window_c.transpose(1, 0, 2),
        head_gain[None],
        ffn_gain[None],
        route_ids.T,
        route_weights.T,
    ]
    large = [
        w_gate_z, w_value_x, w_key_b, w_query_c, w_step.T, state_rows, w_out,
        expert_gate[0], expert_up[0], expert_down[0],
    ]
    operands = [pltpu.with_memory_space_constraint(each, pltpu.HBM) for each in small + large]
    tiles = width // LANES
    n_lines = n_ep * slots * tiles
    n_rows = -(-n_ep * slots // 16) * 16
    exchange = (n_ep * n_tp, slots, tiles, LANES)
    vmem = pltpu.VMEM
    dma = pltpu.SemaphoreType.DMA
    return pl.pallas_call(
        functools.partial(layer_entry, n_ep, n_tp, slots, len(small)),
        out_shape=pltpu.VMEM((seqs, width), BF),
        in_specs=[pl.BlockSpec(memory_space=pl.ANY)] * len(operands),
        out_specs=pl.BlockSpec(memory_space=pltpu.VMEM),
        scratch_shapes=[
            vmem(w_gate_z.shape, BF),
            vmem(w_value_x.shape, BF),
            vmem((features, STATE), BF),
            vmem((features, STATE), BF),
            vmem(w_step.shape[::-1], BF),
            vmem(state_rows.shape, F32),
            vmem(w_out.shape, BF),
            vmem(expert_gate.shape[1:], BF),
            vmem(expert_up.shape[1:], BF),
            vmem(expert_down.shape[1:], BF),
            vmem((n_tp - 1, seqs, width), BF),
            vmem((seqs, features), BF),
            vmem((seqs, STATE), F32),
            vmem((seqs, width), F32),
            vmem((n_tp - 1, seqs, width), BF),
            vmem((n_tp - 1, seqs, width), BF),
            vmem(exchange, BF),
            vmem(exchange, BF),
            vmem((n_tp, n_lines, tiles * seqs), BF),
            vmem((n_tp, tiles * seqs, n_lines), BF),
            vmem((n_tp, tiles * seqs, n_lines), BF),
            vmem((tiles * n_rows, n_lines), BF),
            vmem((n_lines, tiles * n_rows), BF),
            vmem((n_rows, units), F32),
            vmem((n_rows, units), F32),
            vmem((n_rows, units), BF),
            vmem(exchange, BF),
            vmem(exchange, BF),
            dma((9,)),
            dma((seqs // 8,)),
            dma,
            dma((n_tp - 1,)),
            dma,
            dma,
            dma,
            dma((n_tp,)),
            dma,
            dma((n_tp,)),
            pltpu.SemaphoreType.REGULAR((n_ep // 2 - 1, 2)),
            *[vmem(each.shape, each.dtype) for each in small],
            dma((len(small),)),
        ],
        compiler_params=pltpu.CompilerParams(
            collective_id=0, has_side_effects=True, vmem_limit_bytes=60 * 1024 * 1024
        ),
        name="layer",
    )(*operands)


def solution(mesh):
    in_specs = (
        P("ep", "tp"),
        P(),
        P(None, "tp"),
        P(None, "tp"),
        P(),
        P(),
        P(),
        P(),
        P(),
        P(),
        P(None, "tp"),
        P(),
        P(),
        P("ep", None, "tp"),
        P("ep", None, None),
        P("ep", None, None),
        P("ep", "tp", None, None),
        P("tp"),
        P("tp", None),
        P(),
        P("ep", None),
        P("ep", None),
        P("ep", None, "tp"),
        P("ep", None, "tp"),
        P("ep", "tp", None),
    )
    out_specs = P("ep", "tp")
    return jax.shard_map(local, mesh=mesh, in_specs=in_specs, out_specs=out_specs, check_vma=False)
```

```python
import functools

import jax
import jax.numpy as jnp
from jax import lax
from jax.experimental import pallas as pl
from jax.experimental.pallas import tpu as pltpu
from jax.sharding import PartitionSpec as P

HEADS = 32
HEAD_DIM = 64
STATE = 128
GROUPS = 2
EXP_IN = 4


norm_epsilon = 1e-06


def row_norm(arr_values, norm_gain):
    widened = arr_values.astype(jnp.float32)
    return (
        widened
        * lax.rsqrt(jnp.mean(widened * widened, axis=-1, keepdims=True) + norm_epsilon)
        * norm_gain
    )


def short_conv(window, fresh_row, weight):
    conv_taps = weight.astype(jnp.float32)
    summed = (
        jnp.sum(window.astype(jnp.float32) * conv_taps[:-1][None], axis=1)
        + fresh_row * conv_taps[-1]
    )
    return jax.nn.silu(summed)


def product(left, right):
    return jnp.dot(left, right, preferred_element_type=jnp.float32)


def local_plain(
    tokens,
    mix_gain,
    w_gate_z,
    w_value_x,
    w_key_b,
    w_query_c,
    w_step,
    step_bias,
    decay_log,
    skip_gain,
    conv_x_weight,
    conv_b_weight,
    conv_c_weight,
    window_x,
    window_b,
    window_c,
    ssm_state,
    head_gain,
    w_out,
    ffn_gain,
    route_ids,
    route_weights,
    expert_gate,
    expert_up,
    expert_down,
):
    tp_index = lax.axis_index("tp")
    tp_count = lax.axis_size("tp")
    ep_count = lax.axis_size("ep")
    seq_count = tokens.shape[0]
    gathered = lax.all_gather(tokens, "tp", axis=1, tiled=True)
    normed = row_norm(gathered, mix_gain).astype(jnp.bfloat16)
    local_width = w_gate_z.shape[1]
    head_count = local_width // HEAD_DIM
    first_head = tp_index * head_count
    group_start = first_head // (HEADS // GROUPS) * STATE
    gate_z = product(normed, w_gate_z)
    values = short_conv(window_x, product(normed, w_value_x), conv_x_weight)
    key_b = short_conv(
        lax.dynamic_slice_in_dim(window_b, group_start, STATE, 2),
        product(normed, lax.dynamic_slice_in_dim(w_key_b, group_start, STATE, 1)),
        lax.dynamic_slice_in_dim(conv_b_weight, group_start, STATE, 1),
    )
    query_c = short_conv(
        lax.dynamic_slice_in_dim(window_c, group_start, STATE, 2),
        product(normed, lax.dynamic_slice_in_dim(w_query_c, group_start, STATE, 1)),
        lax.dynamic_slice_in_dim(conv_c_weight, group_start, STATE, 1),
    )
    step_all = product(normed, w_step) + step_bias
    step_size = jax.nn.softplus(lax.dynamic_slice_in_dim(step_all, first_head, head_count, 1))
    rate_heads = jnp.exp(lax.dynamic_slice_in_dim(decay_log, first_head, head_count, 0))
    skip_heads = lax.dynamic_slice_in_dim(skip_gain, first_head, head_count, 0)
    decay_heads = jnp.exp(-step_size * rate_heads)
    value_heads = values.reshape(seq_count, head_count, HEAD_DIM)
    new_state = (
        decay_heads[:, :, None, None] * ssm_state
        + (step_size[:, :, None] * value_heads)[..., None] * key_b[:, None, None, :]
    )
    read_out = jnp.einsum("shpn,sn->shp", new_state, query_c, precision=lax.Precision.HIGHEST)
    read_out = read_out + skip_heads[None, :, None] * value_heads
    gated = read_out * jax.nn.silu(gate_z.reshape(seq_count, head_count, HEAD_DIM))
    gated = gated * lax.rsqrt(jnp.mean(gated * gated, axis=-1, keepdims=True) + norm_epsilon)
    mixed_heads = (
        (gated * head_gain.reshape(head_count, HEAD_DIM))
        .reshape(seq_count, local_width)
        .astype(jnp.bfloat16)
    )
    partial_value = product(mixed_heads, w_out)
    share_mix = lax.psum_scatter(partial_value, "tp", scatter_dimension=1, tiled=True)
    residual_own = (tokens.astype(jnp.float32) + share_mix).astype(jnp.bfloat16)
    residual_full = lax.all_gather(residual_own, "tp", axis=1, tiled=True)
    ffn_in = row_norm(residual_full, ffn_gain).astype(jnp.bfloat16)
    top_count = route_ids.shape[1]
    expert_count = EXP_IN * ep_count
    capacity = max(2, (3 * seq_count * top_count + 2 * expert_count - 1) // (2 * expert_count))
    sub_index = tp_index // (tp_count // EXP_IN)
    target_set = route_ids // EXP_IN
    hit_mask = route_ids % EXP_IN == sub_index
    set_grid = jnp.arange(ep_count, dtype=jnp.int32)
    set_onehot = (hit_mask[:, :, None] & (target_set[:, :, None] == set_grid)).astype(jnp.int32)
    set_onehot = set_onehot.reshape(seq_count * top_count, ep_count)
    earlier = jnp.cumsum(set_onehot, axis=0) - set_onehot
    slot_rank = jnp.sum(earlier * set_onehot, axis=1).reshape(seq_count, top_count)
    slot_index = jnp.where(hit_mask, target_set * capacity + slot_rank, -1)
    slot_grid = jnp.arange(ep_count * capacity, dtype=jnp.int32)
    slot_match = slot_index[:, :, None] == slot_grid
    placed = jnp.any(slot_match, axis=1).astype(jnp.bfloat16)
    outgoing = jnp.einsum("sj,sd->jd", placed, ffn_in, preferred_element_type=jnp.float32)
    outgoing = outgoing.astype(jnp.bfloat16).reshape(ep_count, capacity, ffn_in.shape[1])
    route_share = route_weights / jnp.sum(route_weights, axis=1, keepdims=True)
    combine_weight = jnp.sum(jnp.where(slot_match, route_share[:, :, None], 0.0), axis=1)
    arrived = lax.all_to_all(outgoing, "ep", split_axis=0, concat_axis=0, tiled=True)
    source_count, slot_count, row_width = arrived.shape
    flat_rows = arrived.reshape(source_count * slot_count, row_width)
    gate_part = product(flat_rows, expert_gate[0])
    up_part = product(flat_rows, expert_up[0])
    hidden = (jax.nn.silu(gate_part) * up_part).astype(jnp.bfloat16)
    expert_out = product(hidden, expert_down[0]).reshape(source_count, slot_count, row_width)
    returned = lax.all_to_all(
        expert_out.astype(jnp.bfloat16), "ep", split_axis=0, concat_axis=0, tiled=True
    ).astype(expert_out.dtype)
    moe_part = jnp.dot(
        combine_weight,
        returned.reshape(ep_count * capacity, -1),
        precision=lax.Precision.HIGHEST,
        preferred_element_type=jnp.float32,
    )
    moe_share = lax.psum_scatter(
        moe_part.astype(jnp.bfloat16), "tp", scatter_dimension=1, tiled=True
    ).astype(jnp.float32)
    return (residual_own.astype(jnp.float32) + moe_share).astype(jnp.bfloat16)


MESH = pl.DeviceIdType.MESH
HIGH = lax.Precision.HIGHEST
BF = jnp.bfloat16
F32 = jnp.float32
LANES = 128
TILE = 256
ROW_SEND, ROW_USE = (0, 1, 2, 3), (0, 1, 2, 3)
STATE_BLOCKS = 2


def silu(v):
    return v / (1.0 + jnp.exp(-v))


def dot32(left, right, precision=None):
    return jnp.dot(left, right, preferred_element_type=F32, precision=precision)


def dot32_t(left, right):
    return lax.dot_general(left, right, (((1,), (1,)), ((), ())), preferred_element_type=F32)


def halves(v):
    high = v.astype(BF)
    return high, (v - high.astype(F32)).astype(BF)


def split_index(index, *counts):
    digits = []
    for place in range(len(counts) - 1):
        below = 1
        for count in counts[place + 1 :]:
            below = below * count
        digit = jnp.zeros_like(index)
        for step in range(1, counts[place]):
            digit = digit + jnp.where(index >= step * below, 1, 0)
        index = index - digit * below
        digits.append(digit)
    return (*digits, index)


_open = []


def mark(name):
    if _open:
        _open.pop().__exit__(None, None, None)
    if name:
        scope = jax.named_scope(name)
        scope.__enter__()
        _open.append(scope)


def layer_entry(n_ep, n_tp, slots, n_small, *refs):
    held, small_sem = refs[-1 - n_small : -1], refs[-1]
    fetches = [
        pltpu.make_async_copy(refs[at], held[at], small_sem.at[at]) for at in range(n_small)
    ]
    layer_kernel(n_ep, n_tp, slots, fetches, *held, *refs[n_small : -1 - n_small])


def layer_kernel(
    n_ep,
    n_tp,
    slots,
    fetches,
    tokens,
    mix_gain,
    step_bias,
    decay_log,
    skip_gain,
    conv_x,
    conv_b,
    conv_c,
    window_x,
    window_b,
    window_c,
    head_gain,
    ffn_gain,
    ids_t,
    scores_t,
    hbm_gate_z,
    hbm_value_x,
    hbm_key_b,
    hbm_query_c,
    hbm_step,
    hbm_state,
    hbm_out,
    hbm_exp_gate,
    hbm_exp_up,
    hbm_exp_down,
    out,
    w_gate_z,
    w_value_x,
    w_key_b,
    w_query_c,
    w_step,
    state,
    w_out,
    exp_gate,
    exp_up,
    exp_down,
    gathered,
    normed,
    raw_value,
    raw_gate,
    state_read,
    mix_send,
    mix_recv,
    row_send,
    row_recv,
    place,
    comb_high,
    comb_low,
    pick,
    unpick,
    sum_egate,
    sum_eup,
    hidden,
    back_send,
    back_recv,
    load_sem,
    state_sem,
    tok_send_sem,
    tok_recv_sem,
    mix_send_sem,
    mix_recv_sem,
    row_send_sem,
    row_recv_sem,
    back_send_sem,
    back_recv_sem,
    chain_sem,
):
    me_e = lax.axis_index("ep")
    me_t = lax.axis_index("tp")
    seqs, width = tokens.shape
    features = width * n_tp
    tiles = width // LANES
    n_lines = n_ep * slots * tiles
    n_rows = hidden.shape[0]
    carried = (n_ep, slots, tiles, LANES)
    heads_here = width // HEAD_DIM
    first_head = me_t * heads_here
    group_start = pl.multiple_of(first_head // (HEADS // GROUPS) * STATE, STATE)
    group_cols = pl.ds(group_start, STATE)
    state_blocks = state_sem.shape[0]
    state_rows = seqs // state_blocks

    def peer(step):
        row, column = me_t // 2, lax.rem(me_t, 2)
        return lax.rem(row + step // 2, 2) * 2 + lax.rem(column + step % 2, 2)

    def other_e(step):
        return lax.rem(me_e + step, n_ep)

    far_first = sorted(range(n_ep), key=lambda step: -min(step, n_ep - step))
    steps = tuple(reversed(range(n_tp)))

    def load(source, target, index):
        return pltpu.make_async_copy(source, target, load_sem.at[index])

    load_key = load(hbm_key_b.at[:, group_cols], w_key_b, 0)
    load_query = load(hbm_query_c.at[:, group_cols], w_query_c, 1)
    load_step = load(hbm_step, w_step, 2)
    load_value = load(hbm_value_x, w_value_x, 3)
    load_gate = load(hbm_gate_z, w_gate_z, 4)
    load_out = load(hbm_out, w_out, 5)
    load_exp_gate = load(hbm_exp_gate, exp_gate, 6)
    load_exp_up = load(hbm_exp_up, exp_up, 7)
    load_exp_down = load(hbm_exp_down, exp_down, 8)

    def load_state(block):
        rows = pl.ds(block * state_rows, state_rows)
        return pltpu.make_async_copy(hbm_state.at[rows], state.at[rows], state_sem.at[block])

    mark("greet")
    for each in fetches:
        each.start()
    barrier = pltpu.get_barrier_semaphore()
    for step in range(1, n_tp):
        pl.semaphore_signal(
            barrier, inc=1, device_id=(me_e, peer(step)), device_id_type=MESH
        )
    partner = me_e // 2 * 2 + 1 - lax.rem(me_e, 2)
    has_below = (me_e + n_ep - 2) // n_ep
    has_above = (2 * n_ep - 3 - me_e) // n_ep

    def signal_e(semaphore, to_e):
        pl.semaphore_signal(semaphore, inc=1, device_id=(to_e, me_t), device_id_type=MESH)

    signal_e(barrier, partner)

    @pl.when(has_below == 1)
    def _():
        signal_e(barrier, me_e - 2)

    @pl.when(has_above == 1)
    def _():
        signal_e(barrier, me_e + 2)

    def chain_send(turn):
        @pl.when(has_below == 1)
        def _():
            signal_e(chain_sem.at[turn, 0], me_e - 2)

        @pl.when(has_above == 1)
        def _():
            signal_e(chain_sem.at[turn, 1], me_e + 2)

    def chain_wait(turn):
        @pl.when(has_above == 1)
        def _():
            pl.semaphore_wait(chain_sem.at[turn, 0], 1)

        @pl.when(has_below == 1)
        def _():
            pl.semaphore_wait(chain_sem.at[turn, 1], 1)

    turns = n_ep // 2 - 1

    def turn_on(start, stop):
        for turn in range(start, stop):
            if turn < turns:
                chain_wait(turn - 1)
                chain_send(turn)

    mark("loads")
    for each in (load_query, load_key, load_step, load_value, load_gate):
        each.start()
    for block in range(state_blocks):
        load_state(block).start(priority=1)
    mark("smallwait")
    fetches[0].wait()
    mark("barrier")
    pl.semaphore_wait(barrier, n_tp + has_below + has_above)
    mark("toksend")

    def token_copy(step):
        return pltpu.make_async_remote_copy(
            src_ref=tokens,
            dst_ref=gathered.at[step - 1],
            send_sem=tok_send_sem,
            recv_sem=tok_recv_sem.at[step - 1],
            device_id=(me_e, peer(step)),
            device_id_type=MESH,
        )

    for step in reversed(range(1, n_tp)):
        token_copy(step).start()
    chain_send(0)
    mark("smallrest")
    for each in fetches[1:]:
        each.wait()

    def part_rows(step):
        return pl.ds(pl.multiple_of(peer(step) * width, width), width)

    def squares_of(piece):
        wide = piece.astype(F32)
        return jnp.sum(wide * wide, axis=1, keepdims=True)

    mark("routes")
    n_exp = n_ep * EXP_IN
    row_at = lax.broadcasted_iota(jnp.int32, (seqs, seqs), 0)
    col_at = lax.broadcasted_iota(jnp.int32, (seqs, seqs), 1)

    def stood_up(row):
        return jnp.sum(jnp.where(row_at == col_at, row, 0.0), axis=1, keepdims=True)

    id0 = stood_up(ids_t[0:1, :].astype(F32)).astype(jnp.int32)
    id1 = stood_up(ids_t[1:2, :].astype(F32)).astype(jnp.int32)
    lane_exp = lax.broadcasted_iota(jnp.int32, (seqs, n_exp), 1)
    hit0 = jnp.where(id0 == lane_exp, 1.0, 0.0)
    hit1 = jnp.where(id1 == lane_exp, 1.0, 0.0)
    lower = jnp.where(row_at > col_at, 1.0, 0.0).astype(BF)
    upper = jnp.where(row_at < col_at, 1.0, 0.0).astype(BF)
    before = dot32(lower, (hit0 + hit1).astype(BF))
    slot0 = id0 * slots + jnp.sum(before * hit0, axis=1, keepdims=True).astype(jnp.int32)
    slot1 = id1 * slots + jnp.sum(before * hit1, axis=1, keepdims=True).astype(jnp.int32)
    score0, score1 = stood_up(scores_t[0:1, :]), stood_up(scores_t[1:2, :])
    total = score0 + score1

    def stacked(column):
        return jnp.concatenate([column] * tiles, axis=0)

    slot0, slot1 = stacked(slot0), stacked(slot1)
    share0, share1 = stacked(score0 / total), stacked(score1 / total)

    idt0, idt1 = ids_t[0:1, :], ids_t[1:2, :]
    sub_exp = lax.broadcasted_iota(jnp.int32, (n_exp, seqs), 0)
    hitt0 = jnp.where(idt0 == sub_exp, 1.0, 0.0)
    hitt1 = jnp.where(idt1 == sub_exp, 1.0, 0.0)
    before_t = dot32((hitt0 + hitt1).astype(BF), upper)
    rank0 = jnp.sum(before_t * hitt0, axis=0, keepdims=True)
    rank1 = jnp.sum(before_t * hitt1, axis=0, keepdims=True)
    rep_row = lax.broadcasted_iota(jnp.int32, (seqs, tiles * seqs), 0)
    rep_col = lax.broadcasted_iota(jnp.int32, (1, tiles * seqs), 1)
    tile_col, token_col = split_index(rep_col, tiles, seqs)
    repeat = jnp.where(rep_row == token_col, 1.0, 0.0).astype(BF)
    wide_ids = dot32(
        jnp.concatenate([idt0.astype(F32), idt1.astype(F32), rank0, rank1] * 2, axis=0).astype(BF),
        repeat,
    ).astype(jnp.int32)
    slott0 = wide_ids[0:1, :] * slots + wide_ids[2:3, :]
    slott1 = wide_ids[1:2, :] * slots + wide_ids[3:4, :]

    line_row = lax.broadcasted_iota(jnp.int32, (n_lines, 1), 0)
    e_row, k_row, c_row = split_index(line_row, n_ep, slots, tiles)
    line_col = lax.broadcasted_iota(jnp.int32, (1, n_lines), 1)
    e_col, k_col, c_col = split_index(line_col, n_ep, slots, tiles)
    tok_row = lax.broadcasted_iota(jnp.int32, (tiles * seqs, 1), 0)
    tile_row, _ = split_index(tok_row, tiles, seqs)
    pick_row = lax.broadcasted_iota(jnp.int32, (tiles * n_rows, 1), 0)
    pick[...] = jnp.where(
        pick_row == c_col * n_rows + e_col * slots + k_col, 1.0, 0.0
    ).astype(BF)
    pick_col = lax.broadcasted_iota(jnp.int32, (1, tiles * n_rows), 1)
    unpick[...] = jnp.where(
        pick_col == c_row * n_rows + e_row * slots + k_row, 1.0, 0.0
    ).astype(BF)
    for step in range(n_tp):
        there_row = (e_row * n_tp + peer(step)) * slots + k_row
        there_col = (e_col * n_tp + peer(step)) * slots + k_col
        same = c_row == tile_col
        chosen = same & ((slott0 == there_row) | (slott1 == there_row))
        place[step] = jnp.where(chosen, 1.0, 0.0).astype(BF)
        same = tile_row == c_col
        weight = jnp.where(same & (slot0 == there_col), share0, 0.0) + jnp.where(
            same & (slot1 == there_col), share1, 0.0
        )
        comb_high[step], comb_low[step] = halves(weight)

    mark("pasts")

    def window_sum(window, taps, columns):
        summed = None
        for tap in range(window.shape[0]):
            term = window[tap, :, columns].astype(F32) * taps[tap : tap + 1, :]
            summed = term if summed is None else summed + term
        return summed

    every = pl.ds(0, width)
    taps_x = conv_x[...].astype(F32)
    taps_b = conv_b[:, group_cols].astype(F32)
    taps_c = conv_c[:, group_cols].astype(F32)
    last = taps_x.shape[0] - 1
    past_x = window_sum(window_x, taps_x, every)
    past_b = window_sum(window_b, taps_b, group_cols)
    past_c = window_sum(window_c, taps_c, group_cols)
    head_row = lax.broadcasted_iota(jnp.int32, (HEADS, width), 0)
    head_col = lax.broadcasted_iota(jnp.int32, (HEADS, width), 1) // HEAD_DIM + first_head
    spread = jnp.where(head_row == head_col, 1.0, 0.0).astype(BF)
    same_row = lax.rem(lax.broadcasted_iota(jnp.int32, (2 * LANES, LANES), 0), LANES) // HEAD_DIM
    same_col = lax.broadcasted_iota(jnp.int32, (2 * LANES, LANES), 1) // HEAD_DIM
    same_head = jnp.where(same_row == same_col, 1.0, 0.0).astype(BF)
    skip = dot32(jnp.broadcast_to(skip_gain[...], (8, HEADS)), spread.astype(F32), HIGH)[0:1, :]

    squares = squares_of(tokens[...])
    for step in range(1, n_tp):
        mark(f"tokwait{step}")
        token_copy(step).wait_recv()
        squares = squares + squares_of(gathered[step - 1])
    mark("norm")
    for each in (load_out, load_exp_gate, load_exp_up, load_exp_down):
        each.start(priority=1)
    scale = lax.rsqrt(squares / features + norm_epsilon)
    for step in range(n_tp):
        piece = gathered[step - 1] if step else tokens[...]
        columns = part_rows(step)
        normed[:, columns] = (piece.astype(F32) * scale * mix_gain[:, columns]).astype(BF)
    turn_on(1, 2)
    mark("projwait")
    for each in (load_query, load_key, load_step, load_value, load_gate):
        each.wait()
    mark("query")
    query = silu(past_c + dot32(normed[...], w_query_c[...]) * taps_c[last : last + 1, :])
    key = silu(past_b + dot32(normed[...], w_key_b[...]) * taps_b[last : last + 1, :])
    key_query = jnp.sum(key * query, axis=1, keepdims=True)
    raw_step = dot32_t(normed[...], w_step[...]) + step_bias[...]
    step_size = jnp.maximum(raw_step, 0.0) + jnp.log1p(jnp.exp(-jnp.abs(raw_step)))
    decay = jnp.exp(-step_size * jnp.exp(decay_log[...]))
    spread_high, spread_low = halves(jnp.concatenate([step_size, decay], axis=0))
    wide = dot32(jnp.concatenate([spread_high, spread_low], axis=0), spread)
    step_wide = wide[0:seqs] + wide[2 * seqs : 3 * seqs]
    decay_wide = wide[seqs : 2 * seqs] + wide[3 * seqs : 4 * seqs]
    asked = jnp.concatenate([query, jnp.zeros((LANES - seqs, STATE), F32)], axis=0).T
    lane_seq = lax.broadcasted_iota(jnp.int32, (STATE, LANES), 1)
    state_read[...] = jnp.zeros(state_read.shape, F32)
    part_cols = width // state_blocks

    mark("state")

    def read_block(block, carry):
        load_state(block).wait()

        @pl.when(block == state_blocks - 1)
        def _():
            turn_on(2, turns)

        columns = pl.ds(pl.multiple_of(block * part_cols, LANES), part_cols)
        raw_value[:, columns] = dot32(normed[...], w_value_x[:, columns])
        raw_gate[:, columns] = dot32(normed[...], w_gate_z[:, columns])
        found = None
        for pair in range(state_rows // 2):
            first = block * state_rows + pair * 2
            held = jnp.concatenate([state[first], state[first + 1]], axis=1).astype(BF)
            wanted = jnp.concatenate(
                [
                    jnp.where(lane_seq == first, asked, 0.0),
                    jnp.where(lane_seq == first + 1, asked, 0.0),
                ],
                axis=0,
            ).astype(BF)
            part = dot32(held, wanted)
            found = part if found is None else found + part
        state_read[...] = state_read[...] + found
        return carry

    lax.fori_loop(0, state_blocks, read_block, 0)
    mark("values")
    found = state_read[...].T[0:seqs, :]
    values = silu(past_x + raw_value[...] * taps_x[last : last + 1, :])
    direct = values * (step_wide * key_query + skip)
    gate_z = silu(raw_gate[...])

    mark("gated")
    gated = (decay_wide * found + direct) * gate_z
    squared = gated * gated
    squared = jnp.concatenate(
        [squared[:, tile * LANES : (tile + 1) * LANES] for tile in range(tiles)], axis=0
    )
    head_sum = dot32(jnp.concatenate(halves(squared), axis=1), same_head)
    norm = lax.rsqrt(head_sum / HEAD_DIM + norm_epsilon)
    norm = jnp.concatenate(
        [norm[tile * seqs : (tile + 1) * seqs, :] for tile in range(tiles)], axis=1
    )
    mixed = (gated * norm * head_gain[...]).astype(BF)

    mark("outproj")
    chain_wait(turns - 1)
    load_out.wait()

    def mix_copy(step):
        return pltpu.make_async_remote_copy(
            src_ref=mix_send.at[step - 1],
            dst_ref=mix_recv.at[step - 1],
            send_sem=mix_send_sem,
            recv_sem=mix_recv_sem,
            device_id=(me_e, peer(step)),
            device_id_type=MESH,
        )

    def all_mixes():
        return pltpu.make_async_remote_copy(
            src_ref=mix_send,
            dst_ref=mix_recv,
            send_sem=mix_send_sem,
            recv_sem=mix_recv_sem,
            device_id=(me_e, peer(1)),
            device_id_type=MESH,
        )

    for step in steps:
        share = dot32(mixed, w_out[:, part_rows(step)])
        if step:
            mix_send[step - 1] = share.astype(BF)
            mix_copy(step).start()
        else:
            mix_sum = share
    mark("mixwait")
    all_mixes().wait_recv()
    mark("residual")
    for step in range(1, n_tp):
        mix_sum = mix_sum + mix_recv[step - 1].astype(F32)
    residual = (tokens[...].astype(F32) + mix_sum).astype(BF)

    def chunk(step):
        return pl.ds(step * n_ep, n_ep)

    def exchange(send, recv, send_sem, recv_sem, step, step_e):
        return pltpu.make_async_remote_copy(
            src_ref=send.at[step * n_ep + other_e(step_e)],
            dst_ref=recv.at[step * n_ep + me_e],
            send_sem=send_sem,
            recv_sem=recv_sem.at[step],
            device_id=(other_e(step_e), peer(step)),
            device_id_type=MESH,
        )

    def send_out(send, recv, send_sem, recv_sem, step):
        for step_e in far_first:
            if step or step_e:
                exchange(send, recv, send_sem, recv_sem, step, step_e).start()
        if step == 0:
            recv[me_e] = send[me_e]

    def await_chunk(send, recv, send_sem, recv_sem, step):
        blocks = chunk(step) if step else pl.ds(0, n_ep - 1)
        pltpu.make_async_remote_copy(
            src_ref=send.at[blocks],
            dst_ref=recv.at[blocks],
            send_sem=send_sem,
            recv_sem=recv_sem.at[step],
            device_id=(me_e, peer(1)),
            device_id_type=MESH,
        ).wait_recv()

    def await_sent(send, recv, send_sem, recv_sem):
        blocks = pl.ds(0, n_ep * n_tp - 1)
        pltpu.make_async_remote_copy(
            src_ref=send.at[blocks],
            dst_ref=recv.at[blocks],
            send_sem=send_sem,
            recv_sem=recv_sem.at[0],
            device_id=(me_e, peer(1)),
            device_id_type=MESH,
        ).wait_send()

    out_rows = (row_send, row_recv, row_send_sem, row_recv_sem)
    back_rows = (back_send, back_recv, back_send_sem, back_recv_sem)
    stack = jnp.concatenate(
        [residual[:, tile * LANES : (tile + 1) * LANES] for tile in range(tiles)], axis=0
    )
    for step in ROW_SEND:
        mark(f"place{step}")
        outgoing = dot32(place[step], stack).astype(BF)
        row_send[chunk(step)] = outgoing.reshape(carried)
        mark(f"rowsend{step}")
        send_out(*out_rows, step)

    mark("expwait")
    load_exp_gate.wait()
    load_exp_up.wait()
    load_exp_down.wait()
    pltpu.make_async_remote_copy(
        src_ref=gathered,
        dst_ref=gathered,
        send_sem=tok_send_sem,
        recv_sem=tok_recv_sem.at[0],
        device_id=(me_e, peer(1)),
        device_id_type=MESH,
    ).wait_send()
    all_mixes().wait_send()

    units = exp_gate.shape[1]
    squares = jnp.zeros((n_rows, 1), F32)
    for step in ROW_USE:
        mark(f"rowwait{step}")
        await_chunk(*out_rows, step)
        mark(f"gateup{step}")
        came = dot32(pick[...], row_recv[chunk(step)].reshape(n_lines, LANES))
        rows = part_rows(step)
        pieces = [came[tile * n_rows : (tile + 1) * n_rows, :] for tile in range(tiles)]
        for piece in pieces:
            squares = squares + jnp.sum(piece * piece, axis=1, keepdims=True)
        left = (jnp.concatenate(pieces, axis=1) * ffn_gain[:, rows]).astype(BF)
        scale = lax.rsqrt(squares / features + norm_epsilon)
        for at in range(units // TILE):
            columns = slice(at * TILE, (at + 1) * TILE)
            gate_part = dot32(left, exp_gate[rows, columns])
            up_part = dot32(left, exp_up[rows, columns])
            if step != ROW_USE[0]:
                gate_part = sum_egate[:, columns] + gate_part
                up_part = sum_eup[:, columns] + up_part
            if step != ROW_USE[-1]:
                sum_egate[:, columns] = gate_part
                sum_eup[:, columns] = up_part
            else:
                hidden[:, columns] = (silu(gate_part * scale) * (up_part * scale)).astype(BF)
    mark("down")

    def expert_part(step):
        result = dot32(hidden[...], exp_down[:, part_rows(step)])
        return jnp.concatenate(
            [result[:, tile * LANES : (tile + 1) * LANES] for tile in range(tiles)], axis=0
        ).astype(BF)

    part = expert_part(steps[0])
    for at, step in enumerate(steps):
        ready = part
        if at + 1 < n_tp:
            part = expert_part(steps[at + 1])
        back_send[chunk(step)] = dot32(unpick[...], ready).astype(BF).reshape(carried)
        send_out(*back_rows, step)
    mark("rowdrain")
    await_sent(*out_rows)
    moe_sum = jnp.zeros((tiles * seqs, LANES), F32)
    for step in steps:
        mark(f"backwait{step}")
        await_chunk(*back_rows, step)
        mark(f"combine{step}")
        came = back_recv[chunk(step)].reshape(n_lines, LANES)
        moe_sum = moe_sum + dot32(comb_high[step], came) + dot32(comb_low[step], came)
    for tile in range(tiles):
        columns = slice(tile * LANES, (tile + 1) * LANES)
        part = moe_sum[tile * seqs : (tile + 1) * seqs, :]
        out[:, columns] = (residual[:, columns].astype(F32) + part).astype(BF)
    mark("drain")
    await_sent(*back_rows)
    mark(None)


def local(
    tokens,
    mix_gain,
    w_gate_z,
    w_value_x,
    w_key_b,
    w_query_c,
    w_step,
    step_bias,
    decay_log,
    skip_gain,
    conv_x_weight,
    conv_b_weight,
    conv_c_weight,
    window_x,
    window_b,
    window_c,
    ssm_state,
    head_gain,
    w_out,
    ffn_gain,
    route_ids,
    route_weights,
    expert_gate,
    expert_up,
    expert_down,
):
    n_ep, n_tp = lax.axis_size("ep"), lax.axis_size("tp")
    seqs, width = tokens.shape
    features = width * n_tp
    units = expert_gate.shape[2]
    slots = -(-3 * seqs * route_ids.shape[1] // (2 * EXP_IN * n_ep))
    if (
        n_tp != EXP_IN
        or n_tp != 4
        or route_ids.shape[1] != 2
        or width % LANES
        or units % TILE
        or seqs % (2 * STATE_BLOCKS)
        or seqs % 16
        or seqs > LANES
        or width % (LANES * STATE_BLOCKS)
        or n_ep * slots * (width // LANES) % 16
        or n_ep % 2
        or n_ep < 4
        or n_ep * EXP_IN > 256
    ):
        return local_plain(
            tokens, mix_gain, w_gate_z, w_value_x, w_key_b, w_query_c, w_step, step_bias,
            decay_log, skip_gain, conv_x_weight, conv_b_weight, conv_c_weight, window_x,
            window_b, window_c, ssm_state, head_gain, w_out, ffn_gain, route_ids,
            route_weights, expert_gate, expert_up, expert_down,
        )
    state_rows = ssm_state.reshape(seqs, width, STATE)
    small = [
        tokens,
        mix_gain[None],
        step_bias[None],
        decay_log[None],
        skip_gain[None],
        conv_x_weight,
        conv_b_weight,
        conv_c_weight,
        window_x.transpose(1, 0, 2),
        window_b.transpose(1, 0, 2),
        window_c.transpose(1, 0, 2),
        head_gain[None],
        ffn_gain[None],
        route_ids.T,
        route_weights.T,
    ]
    large = [
        w_gate_z, w_value_x, w_key_b, w_query_c, w_step.T, state_rows, w_out,
        expert_gate[0], expert_up[0], expert_down[0],
    ]
    operands = [pltpu.with_memory_space_constraint(each, pltpu.HBM) for each in small + large]
    tiles = width // LANES
    n_lines = n_ep * slots * tiles
    n_rows = -(-n_ep * slots // 16) * 16
    exchange = (n_ep * n_tp, slots, tiles, LANES)
    vmem = pltpu.VMEM
    dma = pltpu.SemaphoreType.DMA
    return pl.pallas_call(
        functools.partial(layer_entry, n_ep, n_tp, slots, len(small)),
        out_shape=pltpu.VMEM((seqs, width), BF),
        in_specs=[pl.BlockSpec(memory_space=pl.ANY)] * len(operands),
        out_specs=pl.BlockSpec(memory_space=pltpu.VMEM),
        scratch_shapes=[
            vmem(w_gate_z.shape, BF),
            vmem(w_value_x.shape, BF),
            vmem((features, STATE), BF),
            vmem((features, STATE), BF),
            vmem(w_step.shape[::-1], BF),
            vmem(state_rows.shape, F32),
            vmem(w_out.shape, BF),
            vmem(expert_gate.shape[1:], BF),
            vmem(expert_up.shape[1:], BF),
            vmem(expert_down.shape[1:], BF),
            vmem((n_tp - 1, seqs, width), BF),
            vmem((seqs, features), BF),
            vmem((seqs, width), F32),
            vmem((seqs, width), F32),
            vmem((width, LANES), F32),
            vmem((n_tp - 1, seqs, width), BF),
            vmem((n_tp - 1, seqs, width), BF),
            vmem(exchange, BF),
            vmem(exchange, BF),
            vmem((n_tp, n_lines, tiles * seqs), BF),
            vmem((n_tp, tiles * seqs, n_lines), BF),
            vmem((n_tp, tiles * seqs, n_lines), BF),
            vmem((tiles * n_rows, n_lines), BF),
            vmem((n_lines, tiles * n_rows), BF),
            vmem((n_rows, units), F32),
            vmem((n_rows, units), F32),
            vmem((n_rows, units), BF),
            vmem(exchange, BF),
            vmem(exchange, BF),
            dma((9,)),
            dma((STATE_BLOCKS,)),
            dma,
            dma((n_tp - 1,)),
            dma,
            dma,
            dma,
            dma((n_tp,)),
            dma,
            dma((n_tp,)),
            pltpu.SemaphoreType.REGULAR((n_ep // 2 - 1, 2)),
            *[vmem(each.shape, each.dtype) for each in small],
            dma((len(small),)),
        ],
        compiler_params=pltpu.CompilerParams(
            collective_id=0, has_side_effects=True, vmem_limit_bytes=60 * 1024 * 1024
        ),
        name="layer",
    )(*operands)


def solution(mesh):
    in_specs = (
        P("ep", "tp"),
        P(),
        P(None, "tp"),
        P(None, "tp"),
        P(),
        P(),
        P(),
        P(),
        P(),
        P(),
        P(None, "tp"),
        P(),
        P(),
        P("ep", None, "tp"),
        P("ep", None, None),
        P("ep", None, None),
        P("ep", "tp", None, None),
        P("tp"),
        P("tp", None),
        P(),
        P("ep", None),
        P("ep", None),
        P("ep", None, "tp"),
        P("ep", None, "tp"),
        P("ep", "tp", None),
    )
    out_specs = P("ep", "tp")
    return jax.shard_map(local, mesh=mesh, in_specs=in_specs, out_specs=out_specs, check_vma=False)
```

```python
import functools

import jax
import jax.numpy as jnp
from jax import lax
from jax.experimental import pallas as pl
from jax.experimental.pallas import tpu as pltpu
from jax.sharding import PartitionSpec as P

HEADS = 32
HEAD_DIM = 64
STATE = 128
GROUPS = 2
EXP_IN = 4


norm_epsilon = 1e-06


def row_norm(arr_values, norm_gain):
    widened = arr_values.astype(jnp.float32)
    return (
        widened
        * lax.rsqrt(jnp.mean(widened * widened, axis=-1, keepdims=True) + norm_epsilon)
        * norm_gain
    )


def short_conv(window, fresh_row, weight):
    conv_taps = weight.astype(jnp.float32)
    summed = (
        jnp.sum(window.astype(jnp.float32) * conv_taps[:-1][None], axis=1)
        + fresh_row * conv_taps[-1]
    )
    return jax.nn.silu(summed)


def product(left, right):
    return jnp.dot(left, right, preferred_element_type=jnp.float32)


def local_plain(
    tokens,
    mix_gain,
    w_gate_z,
    w_value_x,
    w_key_b,
    w_query_c,
    w_step,
    step_bias,
    decay_log,
    skip_gain,
    conv_x_weight,
    conv_b_weight,
    conv_c_weight,
    window_x,
    window_b,
    window_c,
    ssm_state,
    head_gain,
    w_out,
    ffn_gain,
    route_ids,
    route_weights,
    expert_gate,
    expert_up,
    expert_down,
):
    tp_index = lax.axis_index("tp")
    tp_count = lax.axis_size("tp")
    ep_count = lax.axis_size("ep")
    seq_count = tokens.shape[0]
    gathered = lax.all_gather(tokens, "tp", axis=1, tiled=True)
    normed = row_norm(gathered, mix_gain).astype(jnp.bfloat16)
    local_width = w_gate_z.shape[1]
    head_count = local_width // HEAD_DIM
    first_head = tp_index * head_count
    group_start = first_head // (HEADS // GROUPS) * STATE
    gate_z = product(normed, w_gate_z)
    values = short_conv(window_x, product(normed, w_value_x), conv_x_weight)
    key_b = short_conv(
        lax.dynamic_slice_in_dim(window_b, group_start, STATE, 2),
        product(normed, lax.dynamic_slice_in_dim(w_key_b, group_start, STATE, 1)),
        lax.dynamic_slice_in_dim(conv_b_weight, group_start, STATE, 1),
    )
    query_c = short_conv(
        lax.dynamic_slice_in_dim(window_c, group_start, STATE, 2),
        product(normed, lax.dynamic_slice_in_dim(w_query_c, group_start, STATE, 1)),
        lax.dynamic_slice_in_dim(conv_c_weight, group_start, STATE, 1),
    )
    step_all = product(normed, w_step) + step_bias
    step_size = jax.nn.softplus(lax.dynamic_slice_in_dim(step_all, first_head, head_count, 1))
    rate_heads = jnp.exp(lax.dynamic_slice_in_dim(decay_log, first_head, head_count, 0))
    skip_heads = lax.dynamic_slice_in_dim(skip_gain, first_head, head_count, 0)
    decay_heads = jnp.exp(-step_size * rate_heads)
    value_heads = values.reshape(seq_count, head_count, HEAD_DIM)
    new_state = (
        decay_heads[:, :, None, None] * ssm_state
        + (step_size[:, :, None] * value_heads)[..., None] * key_b[:, None, None, :]
    )
    read_out = jnp.einsum("shpn,sn->shp", new_state, query_c, precision=lax.Precision.HIGHEST)
    read_out = read_out + skip_heads[None, :, None] * value_heads
    gated = read_out * jax.nn.silu(gate_z.reshape(seq_count, head_count, HEAD_DIM))
    gated = gated * lax.rsqrt(jnp.mean(gated * gated, axis=-1, keepdims=True) + norm_epsilon)
    mixed_heads = (
        (gated * head_gain.reshape(head_count, HEAD_DIM))
        .reshape(seq_count, local_width)
        .astype(jnp.bfloat16)
    )
    partial_value = product(mixed_heads, w_out)
    share_mix = lax.psum_scatter(partial_value, "tp", scatter_dimension=1, tiled=True)
    residual_own = (tokens.astype(jnp.float32) + share_mix).astype(jnp.bfloat16)
    residual_full = lax.all_gather(residual_own, "tp", axis=1, tiled=True)
    ffn_in = row_norm(residual_full, ffn_gain).astype(jnp.bfloat16)
    top_count = route_ids.shape[1]
    expert_count = EXP_IN * ep_count
    capacity = max(2, (3 * seq_count * top_count + 2 * expert_count - 1) // (2 * expert_count))
    sub_index = tp_index // (tp_count // EXP_IN)
    target_set = route_ids // EXP_IN
    hit_mask = route_ids % EXP_IN == sub_index
    set_grid = jnp.arange(ep_count, dtype=jnp.int32)
    set_onehot = (hit_mask[:, :, None] & (target_set[:, :, None] == set_grid)).astype(jnp.int32)
    set_onehot = set_onehot.reshape(seq_count * top_count, ep_count)
    earlier = jnp.cumsum(set_onehot, axis=0) - set_onehot
    slot_rank = jnp.sum(earlier * set_onehot, axis=1).reshape(seq_count, top_count)
    slot_index = jnp.where(hit_mask, target_set * capacity + slot_rank, -1)
    slot_grid = jnp.arange(ep_count * capacity, dtype=jnp.int32)
    slot_match = slot_index[:, :, None] == slot_grid
    placed = jnp.any(slot_match, axis=1).astype(jnp.bfloat16)
    outgoing = jnp.einsum("sj,sd->jd", placed, ffn_in, preferred_element_type=jnp.float32)
    outgoing = outgoing.astype(jnp.bfloat16).reshape(ep_count, capacity, ffn_in.shape[1])
    route_share = route_weights / jnp.sum(route_weights, axis=1, keepdims=True)
    combine_weight = jnp.sum(jnp.where(slot_match, route_share[:, :, None], 0.0), axis=1)
    arrived = lax.all_to_all(outgoing, "ep", split_axis=0, concat_axis=0, tiled=True)
    source_count, slot_count, row_width = arrived.shape
    flat_rows = arrived.reshape(source_count * slot_count, row_width)
    gate_part = product(flat_rows, expert_gate[0])
    up_part = product(flat_rows, expert_up[0])
    hidden = (jax.nn.silu(gate_part) * up_part).astype(jnp.bfloat16)
    expert_out = product(hidden, expert_down[0]).reshape(source_count, slot_count, row_width)
    returned = lax.all_to_all(
        expert_out.astype(jnp.bfloat16), "ep", split_axis=0, concat_axis=0, tiled=True
    ).astype(expert_out.dtype)
    moe_part = jnp.dot(
        combine_weight,
        returned.reshape(ep_count * capacity, -1),
        precision=lax.Precision.HIGHEST,
        preferred_element_type=jnp.float32,
    )
    moe_share = lax.psum_scatter(
        moe_part.astype(jnp.bfloat16), "tp", scatter_dimension=1, tiled=True
    ).astype(jnp.float32)
    return (residual_own.astype(jnp.float32) + moe_share).astype(jnp.bfloat16)


MESH = pl.DeviceIdType.MESH
HIGH = lax.Precision.HIGHEST
BF = jnp.bfloat16
F32 = jnp.float32
LANES = 128
TILE = 256
ROW_SEND, ROW_USE = (0, 1, 2, 3), (0, 1, 2, 3)
STATE_BLOCKS = 2
GATE_EARLY = 0


def silu(v):
    return v / (1.0 + jnp.exp(-v))


def dot32(left, right, precision=None):
    return jnp.dot(left, right, preferred_element_type=F32, precision=precision)


def dot32_t(left, right):
    return lax.dot_general(left, right, (((1,), (1,)), ((), ())), preferred_element_type=F32)


def halves(v):
    high = v.astype(BF)
    return high, (v - high.astype(F32)).astype(BF)


def split_index(index, *counts):
    digits = []
    for place in range(len(counts) - 1):
        below = 1
        for count in counts[place + 1 :]:
            below = below * count
        digit = jnp.zeros_like(index)
        for step in range(1, counts[place]):
            digit = digit + jnp.where(index >= step * below, 1, 0)
        index = index - digit * below
        digits.append(digit)
    return (*digits, index)


_open = []


def mark(name):
    if _open:
        _open.pop().__exit__(None, None, None)
    if name:
        scope = jax.named_scope(name)
        scope.__enter__()
        _open.append(scope)


def layer_entry(n_ep, n_tp, slots, n_small, *refs):
    held, small_sem = refs[-1 - n_small : -1], refs[-1]
    fetches = [
        pltpu.make_async_copy(refs[at], held[at], small_sem.at[at]) for at in range(n_small)
    ]
    layer_kernel(n_ep, n_tp, slots, fetches, *held, *refs[n_small : -1 - n_small])


def layer_kernel(
    n_ep,
    n_tp,
    slots,
    fetches,
    tokens,
    mix_gain,
    step_bias,
    decay_log,
    skip_gain,
    conv_x,
    conv_b,
    conv_c,
    window_x,
    window_b,
    window_c,
    head_gain,
    ffn_gain,
    ids_t,
    scores_t,
    hbm_gate_z,
    hbm_value_x,
    hbm_key_b,
    hbm_query_c,
    hbm_step,
    hbm_state,
    hbm_out,
    hbm_exp_gate,
    hbm_exp_up,
    hbm_exp_down,
    out,
    w_gate_z,
    w_value_x,
    w_key_b,
    w_query_c,
    w_step,
    state,
    w_out,
    exp_gate,
    exp_up,
    exp_down,
    gathered,
    normed,
    raw_value,
    state_read,
    mix_send,
    mix_recv,
    row_send,
    row_recv,
    place,
    comb_high,
    comb_low,
    pick,
    unpick,
    sum_egate,
    sum_eup,
    hidden,
    back_send,
    back_recv,
    load_sem,
    state_sem,
    tok_send_sem,
    tok_recv_sem,
    mix_send_sem,
    mix_recv_sem,
    row_send_sem,
    row_recv_sem,
    back_send_sem,
    back_recv_sem,
    chain_sem,
):
    me_e = lax.axis_index("ep")
    me_t = lax.axis_index("tp")
    seqs, width = tokens.shape
    features = width * n_tp
    tiles = width // LANES
    n_lines = n_ep * slots * tiles
    n_rows = hidden.shape[0]
    carried = (n_ep, slots, tiles, LANES)
    heads_here = width // HEAD_DIM
    first_head = me_t * heads_here
    group_start = pl.multiple_of(first_head // (HEADS // GROUPS) * STATE, STATE)
    group_cols = pl.ds(group_start, STATE)
    state_blocks = state_sem.shape[0]
    state_rows = seqs // state_blocks

    def peer(step):
        row, column = me_t // 2, lax.rem(me_t, 2)
        return lax.rem(row + step // 2, 2) * 2 + lax.rem(column + step % 2, 2)

    def other_e(step):
        return lax.rem(me_e + step, n_ep)

    far_first = sorted(range(n_ep), key=lambda step: -min(step, n_ep - step))
    steps = tuple(reversed(range(n_tp)))

    def load(source, target, index):
        return pltpu.make_async_copy(source, target, load_sem.at[index])

    load_key = load(hbm_key_b.at[:, group_cols], w_key_b, 0)
    load_query = load(hbm_query_c.at[:, group_cols], w_query_c, 1)
    load_step = load(hbm_step, w_step, 2)
    load_value = load(hbm_value_x, w_value_x, 3)
    load_gate = load(hbm_gate_z, w_gate_z, 4)
    load_out = load(hbm_out, w_out, 5)
    load_exp_gate = load(hbm_exp_gate, exp_gate, 6)
    load_exp_up = load(hbm_exp_up, exp_up, 7)
    load_exp_down = load(hbm_exp_down, exp_down, 8)

    def load_state(block):
        rows = pl.ds(block * state_rows, state_rows)
        return pltpu.make_async_copy(hbm_state.at[rows], state.at[rows], state_sem.at[block])

    mark("greet")
    for each in fetches:
        each.start()
    barrier = pltpu.get_barrier_semaphore()
    for step in range(1, n_tp):
        pl.semaphore_signal(
            barrier, inc=1, device_id=(me_e, peer(step)), device_id_type=MESH
        )
    partner = me_e // 2 * 2 + 1 - lax.rem(me_e, 2)
    has_below = (me_e + n_ep - 2) // n_ep
    has_above = (2 * n_ep - 3 - me_e) // n_ep

    def signal_e(semaphore, to_e):
        pl.semaphore_signal(semaphore, inc=1, device_id=(to_e, me_t), device_id_type=MESH)

    signal_e(barrier, partner)

    @pl.when(has_below == 1)
    def _():
        signal_e(barrier, me_e - 2)

    @pl.when(has_above == 1)
    def _():
        signal_e(barrier, me_e + 2)

    def chain_send(turn):
        @pl.when(has_below == 1)
        def _():
            signal_e(chain_sem.at[turn, 0], me_e - 2)

        @pl.when(has_above == 1)
        def _():
            signal_e(chain_sem.at[turn, 1], me_e + 2)

    def chain_wait(turn):
        @pl.when(has_above == 1)
        def _():
            pl.semaphore_wait(chain_sem.at[turn, 0], 1)

        @pl.when(has_below == 1)
        def _():
            pl.semaphore_wait(chain_sem.at[turn, 1], 1)

    turns = n_ep // 2 - 1

    def turn_on(start, stop):
        for turn in range(start, stop):
            if turn < turns:
                chain_wait(turn - 1)
                chain_send(turn)

    mark("loads")
    for each in (load_query, load_key, load_step, load_value):
        each.start()
    for block in range(state_blocks):
        load_state(block).start(priority=GATE_EARLY)
    load_gate.start(priority=1)
    mark("smallwait")
    fetches[0].wait()
    mark("barrier")
    pl.semaphore_wait(barrier, n_tp + has_below + has_above)
    mark("toksend")

    def token_copy(step):
        return pltpu.make_async_remote_copy(
            src_ref=tokens,
            dst_ref=gathered.at[step - 1],
            send_sem=tok_send_sem,
            recv_sem=tok_recv_sem.at[step - 1],
            device_id=(me_e, peer(step)),
            device_id_type=MESH,
        )

    for step in reversed(range(1, n_tp)):
        token_copy(step).start()
    chain_send(0)
    mark("smallrest")
    for each in fetches[1:]:
        each.wait()

    def part_rows(step):
        return pl.ds(pl.multiple_of(peer(step) * width, width), width)

    def squares_of(piece):
        wide = piece.astype(F32)
        return jnp.sum(wide * wide, axis=1, keepdims=True)

    mark("routes")
    n_exp = n_ep * EXP_IN
    row_at = lax.broadcasted_iota(jnp.int32, (seqs, seqs), 0)
    col_at = lax.broadcasted_iota(jnp.int32, (seqs, seqs), 1)

    def stood_up(row):
        return jnp.sum(jnp.where(row_at == col_at, row, 0.0), axis=1, keepdims=True)

    id0 = stood_up(ids_t[0:1, :].astype(F32)).astype(jnp.int32)
    id1 = stood_up(ids_t[1:2, :].astype(F32)).astype(jnp.int32)
    lane_exp = lax.broadcasted_iota(jnp.int32, (seqs, n_exp), 1)
    hit0 = jnp.where(id0 == lane_exp, 1.0, 0.0)
    hit1 = jnp.where(id1 == lane_exp, 1.0, 0.0)
    lower = jnp.where(row_at > col_at, 1.0, 0.0).astype(BF)
    upper = jnp.where(row_at < col_at, 1.0, 0.0).astype(BF)
    before = dot32(lower, (hit0 + hit1).astype(BF))
    slot0 = id0 * slots + jnp.sum(before * hit0, axis=1, keepdims=True).astype(jnp.int32)
    slot1 = id1 * slots + jnp.sum(before * hit1, axis=1, keepdims=True).astype(jnp.int32)
    score0, score1 = stood_up(scores_t[0:1, :]), stood_up(scores_t[1:2, :])
    total = score0 + score1

    def stacked(column):
        return jnp.concatenate([column] * tiles, axis=0)

    slot0, slot1 = stacked(slot0), stacked(slot1)
    share0, share1 = stacked(score0 / total), stacked(score1 / total)

    idt0, idt1 = ids_t[0:1, :], ids_t[1:2, :]
    sub_exp = lax.broadcasted_iota(jnp.int32, (n_exp, seqs), 0)
    hitt0 = jnp.where(idt0 == sub_exp, 1.0, 0.0)
    hitt1 = jnp.where(idt1 == sub_exp, 1.0, 0.0)
    before_t = dot32((hitt0 + hitt1).astype(BF), upper)
    rank0 = jnp.sum(before_t * hitt0, axis=0, keepdims=True)
    rank1 = jnp.sum(before_t * hitt1, axis=0, keepdims=True)
    rep_row = lax.broadcasted_iota(jnp.int32, (seqs, tiles * seqs), 0)
    rep_col = lax.broadcasted_iota(jnp.int32, (1, tiles * seqs), 1)
    tile_col, token_col = split_index(rep_col, tiles, seqs)
    repeat = jnp.where(rep_row == token_col, 1.0, 0.0).astype(BF)
    wide_ids = dot32(
        jnp.concatenate([idt0.astype(F32), idt1.astype(F32), rank0, rank1] * 2, axis=0).astype(BF),
        repeat,
    ).astype(jnp.int32)
    slott0 = wide_ids[0:1, :] * slots + wide_ids[2:3, :]
    slott1 = wide_ids[1:2, :] * slots + wide_ids[3:4, :]

    line_row = lax.broadcasted_iota(jnp.int32, (n_lines, 1), 0)
    e_row, k_row, c_row = split_index(line_row, n_ep, slots, tiles)
    line_col = lax.broadcasted_iota(jnp.int32, (1, n_lines), 1)
    e_col, k_col, c_col = split_index(line_col, n_ep, slots, tiles)
    tok_row = lax.broadcasted_iota(jnp.int32, (tiles * seqs, 1), 0)
    tile_row, _ = split_index(tok_row, tiles, seqs)
    pick_row = lax.broadcasted_iota(jnp.int32, (tiles * n_rows, 1), 0)
    pick[...] = jnp.where(
        pick_row == c_col * n_rows + e_col * slots + k_col, 1.0, 0.0
    ).astype(BF)
    pick_col = lax.broadcasted_iota(jnp.int32, (1, tiles * n_rows), 1)
    unpick[...] = jnp.where(
        pick_col == c_row * n_rows + e_row * slots + k_row, 1.0, 0.0
    ).astype(BF)
    for step in range(n_tp):
        there_row = (e_row * n_tp + peer(step)) * slots + k_row
        there_col = (e_col * n_tp + peer(step)) * slots + k_col
        same = c_row == tile_col
        chosen = same & ((slott0 == there_row) | (slott1 == there_row))
        place[step] = jnp.where(chosen, 1.0, 0.0).astype(BF)
        same = tile_row == c_col
        weight = jnp.where(same & (slot0 == there_col), share0, 0.0) + jnp.where(
            same & (slot1 == there_col), share1, 0.0
        )
        comb_high[step], comb_low[step] = halves(weight)

    mark("pasts")

    def window_sum(window, taps, columns):
        summed = None
        for tap in range(window.shape[0]):
            term = window[tap, :, columns].astype(F32) * taps[tap : tap + 1, :]
            summed = term if summed is None else summed + term
        return summed

    every = pl.ds(0, width)
    taps_x = conv_x[...].astype(F32)
    taps_b = conv_b[:, group_cols].astype(F32)
    taps_c = conv_c[:, group_cols].astype(F32)
    last = taps_x.shape[0] - 1
    past_x = window_sum(window_x, taps_x, every)
    past_b = window_sum(window_b, taps_b, group_cols)
    past_c = window_sum(window_c, taps_c, group_cols)
    head_row = lax.broadcasted_iota(jnp.int32, (HEADS, width), 0)
    head_col = lax.broadcasted_iota(jnp.int32, (HEADS, width), 1) // HEAD_DIM + first_head
    spread = jnp.where(head_row == head_col, 1.0, 0.0).astype(BF)
    same_row = lax.rem(lax.broadcasted_iota(jnp.int32, (2 * LANES, LANES), 0), LANES) // HEAD_DIM
    same_col = lax.broadcasted_iota(jnp.int32, (2 * LANES, LANES), 1) // HEAD_DIM
    same_head = jnp.where(same_row == same_col, 1.0, 0.0).astype(BF)
    skip = dot32(jnp.broadcast_to(skip_gain[...], (8, HEADS)), spread.astype(F32), HIGH)[0:1, :]

    squares = squares_of(tokens[...])
    for step in range(1, n_tp):
        mark(f"tokwait{step}")
        token_copy(step).wait_recv()
        squares = squares + squares_of(gathered[step - 1])
    mark("norm")
    for each in (load_out, load_exp_gate, load_exp_up, load_exp_down):
        each.start(priority=1)
    scale = lax.rsqrt(squares / features + norm_epsilon)
    for step in range(n_tp):
        piece = gathered[step - 1] if step else tokens[...]
        columns = part_rows(step)
        normed[:, columns] = (piece.astype(F32) * scale * mix_gain[:, columns]).astype(BF)
    turn_on(1, 2)
    mark("projwait")
    for each in (load_query, load_key, load_step, load_value):
        each.wait()
    mark("query")
    query = silu(past_c + dot32(normed[...], w_query_c[...]) * taps_c[last : last + 1, :])
    key = silu(past_b + dot32(normed[...], w_key_b[...]) * taps_b[last : last + 1, :])
    key_query = jnp.sum(key * query, axis=1, keepdims=True)
    raw_step = dot32_t(normed[...], w_step[...]) + step_bias[...]
    step_size = jnp.maximum(raw_step, 0.0) + jnp.log1p(jnp.exp(-jnp.abs(raw_step)))
    decay = jnp.exp(-step_size * jnp.exp(decay_log[...]))
    spread_high, spread_low = halves(jnp.concatenate([step_size, decay], axis=0))
    wide = dot32(jnp.concatenate([spread_high, spread_low], axis=0), spread)
    step_wide = wide[0:seqs] + wide[2 * seqs : 3 * seqs]
    decay_wide = wide[seqs : 2 * seqs] + wide[3 * seqs : 4 * seqs]
    asked = jnp.concatenate([query, jnp.zeros((LANES - seqs, STATE), F32)], axis=0).T
    lane_seq = lax.broadcasted_iota(jnp.int32, (STATE, LANES), 1)
    state_read[...] = jnp.zeros(state_read.shape, F32)
    part_cols = width // state_blocks

    mark("state")

    def read_block(block, carry):
        load_state(block).wait()

        @pl.when(block == state_blocks - 1)
        def _():
            turn_on(2, turns)

        columns = pl.ds(pl.multiple_of(block * part_cols, LANES), part_cols)
        raw_value[:, columns] = dot32(normed[...], w_value_x[:, columns])
        found = None
        for pair in range(state_rows // 2):
            first = block * state_rows + pair * 2
            held = jnp.concatenate([state[first], state[first + 1]], axis=1).astype(BF)
            wanted = jnp.concatenate(
                [
                    jnp.where(lane_seq == first, asked, 0.0),
                    jnp.where(lane_seq == first + 1, asked, 0.0),
                ],
                axis=0,
            ).astype(BF)
            part = dot32(held, wanted)
            found = part if found is None else found + part
        state_read[...] = state_read[...] + found
        return carry

    lax.fori_loop(0, state_blocks, read_block, 0)
    mark("values")
    load_gate.wait()
    gate_z = silu(dot32(normed[...], w_gate_z[...]))
    found = state_read[...].T[0:seqs, :]
    values = silu(past_x + raw_value[...] * taps_x[last : last + 1, :])
    direct = values * (step_wide * key_query + skip)

    mark("gated")
    gated = (decay_wide * found + direct) * gate_z
    squared = gated * gated
    squared = jnp.concatenate(
        [squared[:, tile * LANES : (tile + 1) * LANES] for tile in range(tiles)], axis=0
    )
    head_sum = dot32(jnp.concatenate(halves(squared), axis=1), same_head)
    norm = lax.rsqrt(head_sum / HEAD_DIM + norm_epsilon)
    norm = jnp.concatenate(
        [norm[tile * seqs : (tile + 1) * seqs, :] for tile in range(tiles)], axis=1
    )
    mixed = (gated * norm * head_gain[...]).astype(BF)

    mark("outproj")
    chain_wait(turns - 1)
    load_out.wait()

    def mix_copy(step):
        return pltpu.make_async_remote_copy(
            src_ref=mix_send.at[step - 1],
            dst_ref=mix_recv.at[step - 1],
            send_sem=mix_send_sem,
            recv_sem=mix_recv_sem,
            device_id=(me_e, peer(step)),
            device_id_type=MESH,
        )

    def all_mixes():
        return pltpu.make_async_remote_copy(
            src_ref=mix_send,
            dst_ref=mix_recv,
            send_sem=mix_send_sem,
            recv_sem=mix_recv_sem,
            device_id=(me_e, peer(1)),
            device_id_type=MESH,
        )

    for step in steps:
        share = dot32(mixed, w_out[:, part_rows(step)])
        if step:
            mix_send[step - 1] = share.astype(BF)
            mix_copy(step).start()
        else:
            mix_sum = share
    mark("mixwait")
    all_mixes().wait_recv()
    mark("residual")
    for step in range(1, n_tp):
        mix_sum = mix_sum + mix_recv[step - 1].astype(F32)
    residual = (tokens[...].astype(F32) + mix_sum).astype(BF)

    def chunk(step):
        return pl.ds(step * n_ep, n_ep)

    def exchange(send, recv, send_sem, recv_sem, step, step_e):
        return pltpu.make_async_remote_copy(
            src_ref=send.at[step * n_ep + other_e(step_e)],
            dst_ref=recv.at[step * n_ep + me_e],
            send_sem=send_sem,
            recv_sem=recv_sem.at[step],
            device_id=(other_e(step_e), peer(step)),
            device_id_type=MESH,
        )

    def send_out(send, recv, send_sem, recv_sem, step):
        for step_e in far_first:
            if step or step_e:
                exchange(send, recv, send_sem, recv_sem, step, step_e).start()
        if step == 0:
            recv[me_e] = send[me_e]

    def await_chunk(send, recv, send_sem, recv_sem, step):
        blocks = chunk(step) if step else pl.ds(0, n_ep - 1)
        pltpu.make_async_remote_copy(
            src_ref=send.at[blocks],
            dst_ref=recv.at[blocks],
            send_sem=send_sem,
            recv_sem=recv_sem.at[step],
            device_id=(me_e, peer(1)),
            device_id_type=MESH,
        ).wait_recv()

    def await_sent(send, recv, send_sem, recv_sem):
        blocks = pl.ds(0, n_ep * n_tp - 1)
        pltpu.make_async_remote_copy(
            src_ref=send.at[blocks],
            dst_ref=recv.at[blocks],
            send_sem=send_sem,
            recv_sem=recv_sem.at[0],
            device_id=(me_e, peer(1)),
            device_id_type=MESH,
        ).wait_send()

    out_rows = (row_send, row_recv, row_send_sem, row_recv_sem)
    back_rows = (back_send, back_recv, back_send_sem, back_recv_sem)
    stack = jnp.concatenate(
        [residual[:, tile * LANES : (tile + 1) * LANES] for tile in range(tiles)], axis=0
    )
    for step in ROW_SEND:
        mark(f"place{step}")
        outgoing = dot32(place[step], stack).astype(BF)
        row_send[chunk(step)] = outgoing.reshape(carried)
        mark(f"rowsend{step}")
        send_out(*out_rows, step)

    mark("expwait")
    load_exp_gate.wait()
    load_exp_up.wait()
    load_exp_down.wait()
    pltpu.make_async_remote_copy(
        src_ref=gathered,
        dst_ref=gathered,
        send_sem=tok_send_sem,
        recv_sem=tok_recv_sem.at[0],
        device_id=(me_e, peer(1)),
        device_id_type=MESH,
    ).wait_send()
    all_mixes().wait_send()

    units = exp_gate.shape[1]
    squares = jnp.zeros((n_rows, 1), F32)
    for step in ROW_USE:
        mark(f"rowwait{step}")
        await_chunk(*out_rows, step)
        mark(f"gateup{step}")
        came = dot32(pick[...], row_recv[chunk(step)].reshape(n_lines, LANES))
        rows = part_rows(step)
        pieces = [came[tile * n_rows : (tile + 1) * n_rows, :] for tile in range(tiles)]
        for piece in pieces:
            squares = squares + jnp.sum(piece * piece, axis=1, keepdims=True)
        left = (jnp.concatenate(pieces, axis=1) * ffn_gain[:, rows]).astype(BF)
        scale = lax.rsqrt(squares / features + norm_epsilon)
        for at in range(units // TILE):
            columns = slice(at * TILE, (at + 1) * TILE)
            gate_part = dot32(left, exp_gate[rows, columns])
            up_part = dot32(left, exp_up[rows, columns])
            if step != ROW_USE[0]:
                gate_part = sum_egate[:, columns] + gate_part
                up_part = sum_eup[:, columns] + up_part
            if step != ROW_USE[-1]:
                sum_egate[:, columns] = gate_part
                sum_eup[:, columns] = up_part
            else:
                hidden[:, columns] = (silu(gate_part * scale) * (up_part * scale)).astype(BF)
    mark("down")

    def expert_part(step):
        result = dot32(hidden[...], exp_down[:, part_rows(step)])
        return jnp.concatenate(
            [result[:, tile * LANES : (tile + 1) * LANES] for tile in range(tiles)], axis=0
        ).astype(BF)

    part = expert_part(steps[0])
    for at, step in enumerate(steps):
        ready = part
        if at + 1 < n_tp:
            part = expert_part(steps[at + 1])
        back_send[chunk(step)] = dot32(unpick[...], ready).astype(BF).reshape(carried)
        send_out(*back_rows, step)
    mark("rowdrain")
    await_sent(*out_rows)
    moe_sum = jnp.zeros((tiles * seqs, LANES), F32)
    for step in steps:
        mark(f"backwait{step}")
        await_chunk(*back_rows, step)
        mark(f"combine{step}")
        came = back_recv[chunk(step)].reshape(n_lines, LANES)
        moe_sum = moe_sum + dot32(comb_high[step], came) + dot32(comb_low[step], came)
    for tile in range(tiles):
        columns = slice(tile * LANES, (tile + 1) * LANES)
        part = moe_sum[tile * seqs : (tile + 1) * seqs, :]
        out[:, columns] = (residual[:, columns].astype(F32) + part).astype(BF)
    mark("drain")
    await_sent(*back_rows)
    mark(None)


def local(
    tokens,
    mix_gain,
    w_gate_z,
    w_value_x,
    w_key_b,
    w_query_c,
    w_step,
    step_bias,
    decay_log,
    skip_gain,
    conv_x_weight,
    conv_b_weight,
    conv_c_weight,
    window_x,
    window_b,
    window_c,
    ssm_state,
    head_gain,
    w_out,
    ffn_gain,
    route_ids,
    route_weights,
    expert_gate,
    expert_up,
    expert_down,
):
    n_ep, n_tp = lax.axis_size("ep"), lax.axis_size("tp")
    seqs, width = tokens.shape
    features = width * n_tp
    units = expert_gate.shape[2]
    slots = -(-3 * seqs * route_ids.shape[1] // (2 * EXP_IN * n_ep))
    if (
        n_tp != EXP_IN
        or n_tp != 4
        or route_ids.shape[1] != 2
        or width % LANES
        or units % TILE
        or seqs % (2 * STATE_BLOCKS)
        or seqs % 16
        or seqs > LANES
        or width % (LANES * STATE_BLOCKS)
        or n_ep * slots * (width // LANES) % 16
        or n_ep % 2
        or n_ep < 4
        or n_ep * EXP_IN > 256
    ):
        return local_plain(
            tokens, mix_gain, w_gate_z, w_value_x, w_key_b, w_query_c, w_step, step_bias,
            decay_log, skip_gain, conv_x_weight, conv_b_weight, conv_c_weight, window_x,
            window_b, window_c, ssm_state, head_gain, w_out, ffn_gain, route_ids,
            route_weights, expert_gate, expert_up, expert_down,
        )
    state_rows = ssm_state.reshape(seqs, width, STATE)
    small = [
        tokens,
        mix_gain[None],
        step_bias[None],
        decay_log[None],
        skip_gain[None],
        conv_x_weight,
        conv_b_weight,
        conv_c_weight,
        window_x.transpose(1, 0, 2),
        window_b.transpose(1, 0, 2),
        window_c.transpose(1, 0, 2),
        head_gain[None],
        ffn_gain[None],
        route_ids.T,
        route_weights.T,
    ]
    large = [
        w_gate_z, w_value_x, w_key_b, w_query_c, w_step.T, state_rows, w_out,
        expert_gate[0], expert_up[0], expert_down[0],
    ]
    operands = [pltpu.with_memory_space_constraint(each, pltpu.HBM) for each in small + large]
    tiles = width // LANES
    n_lines = n_ep * slots * tiles
    n_rows = -(-n_ep * slots // 16) * 16
    exchange = (n_ep * n_tp, slots, tiles, LANES)
    vmem = pltpu.VMEM
    dma = pltpu.SemaphoreType.DMA
    return pl.pallas_call(
        functools.partial(layer_entry, n_ep, n_tp, slots, len(small)),
        out_shape=pltpu.VMEM((seqs, width), BF),
        in_specs=[pl.BlockSpec(memory_space=pl.ANY)] * len(operands),
        out_specs=pl.BlockSpec(memory_space=pltpu.VMEM),
        scratch_shapes=[
            vmem(w_gate_z.shape, BF),
            vmem(w_value_x.shape, BF),
            vmem((features, STATE), BF),
            vmem((features, STATE), BF),
            vmem(w_step.shape[::-1], BF),
            vmem(state_rows.shape, F32),
            vmem(w_out.shape, BF),
            vmem(expert_gate.shape[1:], BF),
            vmem(expert_up.shape[1:], BF),
            vmem(expert_down.shape[1:], BF),
            vmem((n_tp - 1, seqs, width), BF),
            vmem((seqs, features), BF),
            vmem((seqs, width), F32),
            vmem((width, LANES), F32),
            vmem((n_tp - 1, seqs, width), BF),
            vmem((n_tp - 1, seqs, width), BF),
            vmem(exchange, BF),
            vmem(exchange, BF),
            vmem((n_tp, n_lines, tiles * seqs), BF),
            vmem((n_tp, tiles * seqs, n_lines), BF),
            vmem((n_tp, tiles * seqs, n_lines), BF),
            vmem((tiles * n_rows, n_lines), BF),
            vmem((n_lines, tiles * n_rows), BF),
            vmem((n_rows, units), F32),
            vmem((n_rows, units), F32),
            vmem((n_rows, units), BF),
            vmem(exchange, BF),
            vmem(exchange, BF),
            dma((9,)),
            dma((STATE_BLOCKS,)),
            dma,
            dma((n_tp - 1,)),
            dma,
            dma,
            dma,
            dma((n_tp,)),
            dma,
            dma((n_tp,)),
            pltpu.SemaphoreType.REGULAR((n_ep // 2 - 1, 2)),
            *[vmem(each.shape, each.dtype) for each in small],
            dma((len(small),)),
        ],
        compiler_params=pltpu.CompilerParams(
            collective_id=0, has_side_effects=True, vmem_limit_bytes=60 * 1024 * 1024
        ),
        name="layer",
    )(*operands)


def solution(mesh):
    in_specs = (
        P("ep", "tp"),
        P(),
        P(None, "tp"),
        P(None, "tp"),
        P(),
        P(),
        P(),
        P(),
        P(),
        P(),
        P(None, "tp"),
        P(),
        P(),
        P("ep", None, "tp"),
        P("ep", None, None),
        P("ep", None, None),
        P("ep", "tp", None, None),
        P("tp"),
        P("tp", None),
        P(),
        P("ep", None),
        P("ep", None),
        P("ep", None, "tp"),
        P("ep", None, "tp"),
        P("ep", "tp", None),
    )
    out_specs = P("ep", "tp")
    return jax.shard_map(local, mesh=mesh, in_specs=in_specs, out_specs=out_specs, check_vma=False)
```
